32 devices in a mesh: sp: 8 (over z, x), tp: 4 (over y, core).
Axes of the slice: x: 2, y: 2, z: 4, core: 2. Of those that a mesh axis runs over, the one named last changes fastest.
Arguments:
- queries: bfloat16 [4096, 512], P('sp', 'tp'), may hold values from -16 to 16
- key_heads: bfloat16 [4096, 512], P('sp', 'tp'), may hold values from -16 to 16
- value_heads: bfloat16 [4096, 512], P('sp', 'tp'), may hold values from -6 to 6
- head_gain: float32 [512], P('tp'), may hold values from 0.1 to 1.9
- residual: bfloat16 [4096, 2048], P(('sp', 'tp')), may hold values from -6 to 6
- out_weight: bfloat16 [512, 2048], replicated, may hold values from -0.25 to 0.25
- norm_gain: float32 [2048], replicated, may hold values from 0.1 to 1.9
- shared_gate: bfloat16 [2048, 512], replicated, may hold values from -0.125 to 0.125
- shared_up: bfloat16 [2048, 512], replicated, may hold values from -0.125 to 0.125
- shared_down: bfloat16 [512, 2048], replicated, may hold values from -0.25 to 0.25
- expert_gate: bfloat16 [64, 2048, 512], P(('sp', 'tp')), may hold values from -0.125 to 0.125
- expert_up: bfloat16 [64, 2048, 512], P(('sp', 'tp')), may hold values from -0.125 to 0.125
- expert_down: bfloat16 [64, 512, 2048], P(('sp', 'tp')), may hold values from -0.25 to 0.25
- routed_experts: int32 [4096, 4], P(('sp', 'tp')), may hold values from 0 to 63, all different within a row; in each aligned block of 128 rows (0 to 127, 128 to 255, ...) at most 12 rows name the same one
- route_weights: float32 [4096, 4], P(('sp', 'tp')), may hold values from 0.1 to 1.5
Outputs:
- layer_output: bfloat16 [4096, 2048], P(('sp', 'tp'))
The draws below stay inside these ranges and needn't reach their ends.
Inputs may be any that keep to these rules, and one draw needn't show every extreme that they name: `routed_experts`: each row names 4 different experts. Within the rows of one device (128 consecutive rows, aligned) no expert is named more than 12 times, and in every draw some expert is named exactly 12 times in some device's rows.
All inputs are finite; a program needn't handle non-finite values.
Results may differ from the reference program's by a relative error of at most 0.014.
Values may be sent and summed in bfloat16 or wider, within the bound.
A program may use at most 128 MiB of HBM per device.

```python
import math
import jax
import jax.numpy as jnp
import numpy as np
from jax import lax

D = 2048
HEADS = 8
HEAD_DIM = 64
FFE = 512
SHARED_FF = 512
TOPK = 4
TOK_DEV = 128
TOK_SP = 512
TOKEN_COUNT = 4096
EXPERTS = 64
CAP = 12
N_SP = 8
N_TP = 4


def head_law(key):
    base_key = jax.random.fold_in(key, 11)
    direction_key, choice_key, quick_key, gentle_key = jax.random.split(base_key, 4)
    direction = jax.random.normal(direction_key, (HEADS, HEAD_DIM), jnp.float32)
    direction = direction / jnp.sqrt(jnp.sum(direction * direction, axis=1, keepdims=True))
    gentle_share = 0.5
    gentle = jax.random.uniform(choice_key, (HEADS,), jnp.float32) < gentle_share
    quick_rate = jnp.exp(jax.random.uniform(quick_key, (HEADS,), jnp.float32, math.log(3.3), math.log(4.6)))
    gentle_rate = math.log(TOKEN_COUNT) + jax.random.uniform(gentle_key, (HEADS,), jnp.float32, 0.0, 0.8)
    intensity = jnp.where(gentle, gentle_rate, quick_rate)
    return (direction, intensity)


def draw_queries(key, part):
    direction, intensity = head_law(key)
    noise = jnp.clip(jax.random.normal(jax.random.fold_in(key, 21), (TOKEN_COUNT, HEADS, HEAD_DIM), jnp.float32), -3.0, 3.0)
    lifted = jnp.sqrt(intensity * math.sqrt(HEAD_DIM))
    drawn = 0.5 * noise + lifted[None, :, None] * direction[None]
    return drawn.reshape(TOKEN_COUNT, HEADS * HEAD_DIM).astype(jnp.bfloat16)


def draw_key_heads(key, part):
    direction, intensity = head_law(key)
    jitter_random_key, shift_random_key, spike_random_key = jax.random.split(jax.random.fold_in(key, 31), 3)
    noise = jnp.clip(jax.random.normal(jitter_random_key, (TOKEN_COUNT, HEADS, HEAD_DIM), jnp.float32), -3.0, 3.0)
    shift_values = jax.random.uniform(shift_random_key, (TOKEN_COUNT // TOK_SP,), jnp.float32, -0.5, 0.5)
    shift_values = jnp.repeat(shift_values, TOK_SP)
    spike_amount = jax.random.uniform(spike_random_key, (TOKEN_COUNT,), jnp.float32) < 6.0 / TOKEN_COUNT
    lifted = jnp.sqrt(intensity * math.sqrt(HEAD_DIM))
    multiplier = jnp.where(spike_amount[:, None], 0.8 / intensity[None, :], 1.0 + shift_values[:, None] / intensity[None, :])
    drawn = 0.5 * noise - (lifted[None, :] * multiplier)[:, :, None] * direction[None]
    return drawn.reshape(TOKEN_COUNT, HEADS * HEAD_DIM).astype(jnp.bfloat16)


def levels(rng, extent, cuts, least, high):
    factor_of, own = 1.0, jax.random.fold_in(rng, 6)
    for position, shards_of in cuts:
        heights = jnp.exp(jax.random.uniform(jax.random.fold_in(own, position), (shards_of,), jnp.float32, least / len(cuts), high / len(cuts)))
        factor_of = factor_of * jnp.repeat(heights, extent[position] // shards_of).reshape([-1 if axis == position else 1 for axis in range(len(extent))])
    return factor_of


def assign_block(key, own, number, rows, number_of, top, reach, skew):
    order = jax.random.permutation(key, number_of)
    heavy_load, usual = load_shares(number_of, rows * top, reach, skew, True), load_shares(number_of, rows * top, reach, skew, False)
    places = jnp.arange(number_of)

    def named(tallies, turn):
        used = int((tallies > 0).sum())
        fixed = max(1, used // 4)
        shifted = fixed + (places - fixed + turn * (used - fixed)) % max(1, number_of - fixed)
        return jnp.zeros((number_of,), jnp.int32).at[order[jnp.where(places < fixed, places, shifted)]].set(jnp.asarray(tallies, jnp.int32))

    tallies = jnp.where(number % 4 == 0, named(heavy_load, number // 4), named(usual, number - number // 4 - 1))
    mixed = jax.random.permutation(jax.random.fold_in(own, 3), number_of)
    source_of, receiver = mixed[0:number_of // 2 * 2:2], mixed[1:number_of // 2 * 2:2]
    room = jnp.minimum(tallies[source_of] - 1, reach - tallies[receiver]) // 2
    room = jnp.where((source_of == order[0]) | (receiver == order[0]) | (tallies[receiver] == 0), 0, jnp.maximum(room, 0))
    shifted = jax.random.randint(jax.random.fold_in(own, 4), (number_of // 2,), 0, 1 << 20) % (room + 1)
    tallies = tallies.at[source_of].add(-shifted).at[receiver].add(shifted)
    labels = jnp.searchsorted(jnp.cumsum(tallies), jnp.arange(rows * top), side="right").astype(jnp.int32)
    grid = labels.reshape(top, rows).T
    grid = grid[jax.random.permutation(jax.random.fold_in(own, 1), rows)]
    turn = jax.random.randint(jax.random.fold_in(own, 2), (rows, 1), 0, top)
    return jnp.take_along_axis(grid, (jnp.arange(top)[None, :] + turn) % top, axis=1)


def load_shares(number_of, total, bound, lean, full):
    loads = [(1 << 20) // math.isqrt(rank ** lean) + 1 for rank in range(1, number_of + 1)]
    largest = bound if full else min(bound, max(-(-total // number_of), total * loads[0] // sum(loads)))
    least = 1 if total - largest >= number_of - 1 else 0
    holding, rest = [largest] + [least] * (number_of - 1), total - largest - least * (number_of - 1)
    while rest > 0:
        free = [i for i in range(1, number_of) if holding[i] < largest] or [i for i in range(1, number_of) if holding[i] < bound]
        pool, left = sum([loads[i] for i in free]), rest
        for i in free:
            extra = min(bound - holding[i], max(1, left * loads[i] // pool), rest)
            holding[i] = holding[i] + extra
            rest = rest - extra
    return np.array(holding)


def gaussian(rng, extent, scale, limit, cuts=(), kind=jnp.bfloat16):
    result = scale * jax.random.normal(rng, extent, jnp.float32)
    if cuts:
        result = result * levels(rng, extent, cuts, -0.22, 0.18)
    return jnp.clip(result, -limit, limit).astype(kind)


def setup_inputs(seed: int = 0) -> dict:
    key_of = jax.random.split(jax.random.key(seed), 16)
    queries = draw_queries(jax.random.fold_in(key_of[15], 71), 0)
    key_heads = draw_key_heads(jax.random.fold_in(key_of[15], 71), 0)
    value_heads = gaussian(key_of[2], (TOKEN_COUNT, HEADS * HEAD_DIM), 1.0, 6.0, ((0, 8), (1, 4)))
    head_gain = jnp.clip(1.0 + 0.18 * jax.random.normal(key_of[3], (HEADS * HEAD_DIM,), jnp.float32), 0.1, 1.9)
    residual = gaussian(key_of[4], (TOKEN_COUNT, D), 1.0, 6.0, ((0, 32),))
    out_weight = gaussian(key_of[5], (HEADS * HEAD_DIM, D), (HEADS * HEAD_DIM) ** -0.5, 0.25)
    norm_gain = jnp.clip(1.0 + 0.18 * jax.random.normal(key_of[6], (D,), jnp.float32), 0.1, 1.9)
    shared_gate = gaussian(key_of[7], (D, SHARED_FF), D ** -0.5, 0.125)
    shared_up = gaussian(key_of[8], (D, SHARED_FF), D ** -0.5, 0.125)
    shared_down = gaussian(key_of[9], (SHARED_FF, D), SHARED_FF ** -0.5, 0.25)
    expert_gate = gaussian(key_of[10], (EXPERTS, D, FFE), D ** -0.5, 0.125, ((0, 32),))
    expert_up = gaussian(key_of[11], (EXPERTS, D, FFE), D ** -0.5, 0.125, ((0, 32),))
    expert_down = gaussian(key_of[12], (EXPERTS, FFE, D), FFE ** -0.5, 0.25, ((0, 32),))
    routed_experts_keys = jax.random.split(jax.random.fold_in(key_of[13], 1), TOKEN_COUNT // TOK_DEV)
    routed_experts_turns = jax.random.permutation(jax.random.fold_in(key_of[13], 3), TOKEN_COUNT // TOK_DEV)
    routed_experts = jax.vmap(lambda own, number: assign_block(jax.random.fold_in(key_of[13], 2), own, number, TOK_DEV, EXPERTS, TOPK, CAP, 2))(routed_experts_keys, routed_experts_turns).reshape((TOKEN_COUNT, TOPK))
    route_weights = jnp.clip(jnp.exp(math.log(1.5) - 2.7080502 * jax.random.uniform(key_of[14], (TOKEN_COUNT, TOPK), jnp.float32) ** levels(key_of[14], (TOKEN_COUNT, TOPK), ((0, 32),), -0.2, 0.2)), 0.1, 1.5)
    return dict(queries=queries, key_heads=key_heads, value_heads=value_heads, head_gain=head_gain, residual=residual, out_weight=out_weight, norm_gain=norm_gain, shared_gate=shared_gate, shared_up=shared_up, shared_down=shared_down, expert_gate=expert_gate, expert_up=expert_up, expert_down=expert_down, routed_experts=routed_experts, route_weights=route_weights)


EPSILON = 1e-06

def block_terms(query_block, key_block, value_block, query_start, key_start):
    scale = 1.0 / math.sqrt(HEAD_DIM)
    scores = jnp.einsum('qhd,khd->hqk', query_block.astype(jnp.float32), key_block.astype(jnp.float32)) * scale
    query_places = query_start + lax.iota(jnp.int32, query_block.shape[0])
    key_places = key_start + lax.iota(jnp.int32, key_block.shape[0])
    earlier = (key_places[None, :] < query_places[:, None])[None]
    stay_log = jnp.where(earlier, jax.nn.log_sigmoid(-scores), 0.0)
    after_log = lax.cumsum(stay_log, axis=2, reverse=True) - stay_log
    weights = jnp.where(earlier, jnp.exp(jax.nn.log_sigmoid(scores) + after_log), 0.0).astype(jnp.bfloat16)
    partial_out = jnp.einsum('hqk,khd->qhd', weights.astype(jnp.float32), value_block.astype(jnp.float32))
    block_total = jnp.transpose(lax.optimization_barrier(jnp.sum(stay_log, axis=2)))
    return (block_total, partial_out)

def head_norm(mixed, head_gain):
    inverse = lax.rsqrt(lax.optimization_barrier(jnp.mean(mixed * mixed, axis=2, keepdims=True)) + EPSILON)
    normed = mixed * inverse * head_gain.reshape(mixed.shape[1], mixed.shape[2])
    return normed.reshape(mixed.shape[0], -1).astype(jnp.bfloat16)

def stick_breaking(queries, key_heads, value_heads):
    query_width = 512 if TOK_SP % 512 == 0 else TOK_SP
    query_all = queries.reshape(TOKEN_COUNT // query_width, query_width, HEADS, HEAD_DIM)
    key_all = key_heads.reshape(N_SP, TOK_SP, HEADS, HEAD_DIM)
    value_all = value_heads.reshape(N_SP, TOK_SP, HEADS, HEAD_DIM)

    def one_block(block_index):
        query_block = lax.dynamic_index_in_dim(query_all, block_index, 0, keepdims=False)
        query_start = block_index * query_width

        def one_shard(running, shard_index):
            key_start = shard_index * TOK_SP

            def compute(unused):
                key_block = lax.dynamic_index_in_dim(key_all, shard_index, 0, keepdims=False)
                value_block = lax.dynamic_index_in_dim(value_all, shard_index, 0, keepdims=False)
                return block_terms(query_block, key_block, value_block, query_start, key_start)

            def nothing(unused):
                return (jnp.zeros((query_width, HEADS), jnp.float32), jnp.zeros((query_width, HEADS, HEAD_DIM), jnp.float32))
            return (running, lax.cond(key_start < query_start + query_width, compute, nothing, 0))
        leftover, stacked = lax.scan(one_shard, jnp.int32(0), jnp.arange(N_SP, dtype=jnp.int32))
        totals, partials = stacked
        later = lax.cumsum(totals, axis=0, reverse=True) - totals
        return lax.optimization_barrier(jnp.sum(jnp.exp(later)[..., None] * partials, axis=0))
    mixed = lax.map(one_block, jnp.arange(TOKEN_COUNT // query_width, dtype=jnp.int32))
    return mixed.reshape(TOKEN_COUNT, HEADS, HEAD_DIM)

def expert_block(inputs):
    expert_rows, gate_weight, up_weight, down_weight = inputs
    gate_part = jnp.dot(expert_rows, gate_weight, preferred_element_type=jnp.float32)
    up_part = jnp.dot(expert_rows, up_weight, preferred_element_type=jnp.float32)
    hidden = (jax.nn.silu(gate_part) * up_part).astype(jnp.bfloat16)
    return jnp.dot(hidden, down_weight, preferred_element_type=jnp.float32).astype(jnp.bfloat16)

def routed_sum(expert_input, expert_gate, expert_up, expert_down, routed_experts, route_weights):
    device_count = N_SP * N_TP
    flat_experts = routed_experts.reshape(-1)
    expert_table = (flat_experts[:, None] == jnp.arange(EXPERTS, dtype=jnp.int32)[None, :]).astype(jnp.int32)
    expert_table = expert_table.reshape(device_count, TOK_DEV * TOPK, EXPERTS)
    ranking = (lax.optimization_barrier(jnp.sum(jnp.cumsum(expert_table, axis=1) * expert_table, axis=2)) - 1).reshape(-1)
    source = jnp.arange(TOKEN_COUNT * TOPK, dtype=jnp.int32) // (TOK_DEV * TOPK)
    slot_index = (flat_experts * device_count + source) * CAP + ranking
    repeated = jnp.repeat(expert_input, TOPK, axis=0)
    buffer = jnp.zeros((EXPERTS * device_count * CAP, D), jnp.bfloat16).at[slot_index].set(repeated)
    buffer = buffer.reshape(EXPERTS, device_count * CAP, D)
    results = lax.map(expert_block, (buffer, expert_gate, expert_up, expert_down)).reshape(-1, D)
    slot_grid = slot_index.reshape(TOKEN_COUNT, TOPK)
    routed = jnp.zeros((TOKEN_COUNT, D), jnp.float32)
    for choice_index in range(TOPK):
        picked = results[slot_grid[:, choice_index]].astype(jnp.float32)
        routed = routed + picked * route_weights[:, choice_index][:, None]
    return routed

def reference(queries, key_heads, value_heads, head_gain, residual, out_weight, norm_gain, shared_gate, shared_up, shared_down, expert_gate, expert_up, expert_down, routed_experts, route_weights):
    head_output = head_norm(stick_breaking(queries, key_heads, value_heads), head_gain)
    branch = jnp.dot(head_output, out_weight, preferred_element_type=jnp.float32)
    stream = (residual.astype(jnp.float32) + branch).astype(jnp.bfloat16)
    stream_wide = stream.astype(jnp.float32)
    inverse = lax.rsqrt(lax.optimization_barrier(jnp.mean(stream_wide * stream_wide, axis=1, keepdims=True)) + EPSILON)
    expert_input = (stream_wide * inverse * norm_gain).astype(jnp.bfloat16)
    shared_hidden = (jax.nn.silu(jnp.dot(expert_input, shared_gate, preferred_element_type=jnp.float32)) * jnp.dot(expert_input, shared_up, preferred_element_type=jnp.float32)).astype(jnp.bfloat16)
    shared_term = jnp.dot(shared_hidden, shared_down, preferred_element_type=jnp.float32)
    routed = routed_sum(expert_input, expert_gate, expert_up, expert_down, routed_experts, route_weights)
    return (stream_wide + shared_term + routed).astype(jnp.bfloat16)
```

```python
import functools
import math

import jax
import jax.numpy as jnp
from jax import lax
from jax.experimental import pallas as pl
from jax.experimental.pallas import tpu as pltpu
from jax.sharding import PartitionSpec as P

HEAD_DIM = 64


EPSILON = 1e-06

COLUMNS = 2
TILE = 256
LOG2E = 1.4426950408889634
MESH = pl.DeviceIdType.MESH
CHUNKS = 8
LAG = 2
VMEM_LIMIT = 67043328


def attention_kernel(rows, q_ref, kv_ref, gain_ref, out_ref, held, masked, acc, carry, up_send, up_recv, side_send, side_recv):
    me = lax.axis_index("sp")
    row, col = me // COLUMNS, me % COLUMNS
    seq, width = q_ref.shape
    heads = width // HEAD_DIM
    tile = min(TILE, seq)
    tiles = seq // tile
    other = row * COLUMNS + (COLUMNS - 1 - col)

    barrier = pltpu.get_barrier_semaphore()

    @pl.when(row < rows - 1)
    def _():
        pl.semaphore_signal(barrier, inc=1, device_id={"sp": me + COLUMNS}, device_id_type=MESH)

    @pl.when(row > 0)
    def _():
        pl.semaphore_signal(barrier, inc=1, device_id={"sp": me - COLUMNS}, device_id_type=MESH)

    pl.semaphore_signal(barrier, inc=1, device_id={"sp": other}, device_id_type=MESH)
    inner = (row > 0) & (row < rows - 1)

    @pl.when(inner)
    def _():
        pl.semaphore_wait(barrier, 3)

    @pl.when(jnp.logical_not(inner))
    def _():
        pl.semaphore_wait(barrier, min(rows, 2))

    def up_copy(source, depth):
        place = (row - depth) * COLUMNS + col
        return pltpu.make_async_remote_copy(
            src_ref=source, dst_ref=held.at[place], send_sem=up_send.at[depth], recv_sem=up_recv.at[depth],
            device_id={"sp": me + COLUMNS}, device_id_type=MESH)

    def side_copy(source, depth):
        place = (row - depth) * COLUMNS + col
        return pltpu.make_async_remote_copy(
            src_ref=source, dst_ref=held.at[place], send_sem=side_send.at[depth], recv_sem=side_recv.at[depth],
            device_id={"sp": other}, device_id_type=MESH)

    @pl.when(row < rows - 1)
    def _():
        up_copy(kv_ref, 0).start()

    @pl.when(col == 0)
    def _():
        side_copy(kv_ref, 0).start()

    lane = lax.broadcasted_iota(jnp.int32, (1, width), 1) // HEAD_DIM
    key_row = lax.broadcasted_iota(jnp.int32, (tile, tile), 0)
    key_col = lax.broadcasted_iota(jnp.int32, (tile, tile), 1)
    later = (key_row > key_col).astype(jnp.bfloat16)
    scale = LOG2E / math.sqrt(HEAD_DIM)

    for head in range(heads):
        for query_tile in range(tiles):
            source_rows = slice(query_tile * tile, (query_tile + 1) * tile)
            stacked_rows = slice((query_tile * heads + head) * tile, (query_tile * heads + head + 1) * tile)
            masked[stacked_rows, :] = jnp.where(lane == head, q_ref[source_rows, :], jnp.zeros((), q_ref.dtype))

    def span(source, key_tile, first, last, diagonal):
        stacked_rows = slice(first * heads * tile, last * heads * tile)
        key_rows = slice(key_tile * tile, (key_tile + 1) * tile)
        keys = source[key_rows, :width]
        values = source[key_rows, width:]
        scores = lax.dot_general(masked[stacked_rows, :], keys, (((1,), (1,)), ((), ())), preferred_element_type=jnp.float32) * scale
        soft = jnp.log2(1.0 + jnp.exp2(-jnp.abs(scores)))
        take = jnp.minimum(scores, 0.0) - soft
        stay = take - scores
        if diagonal:
            query_place = jnp.concatenate([key_row] * ((last - first) * heads), axis=0)
            key_place = jnp.concatenate([key_col] * ((last - first) * heads), axis=0)
            stay = jnp.where(key_place < query_place, stay, 0.0)
        high = stay.astype(jnp.bfloat16)
        low = (stay - high.astype(jnp.float32)).astype(jnp.bfloat16)
        after = jnp.dot(high, later, preferred_element_type=jnp.float32) + jnp.dot(low, later, preferred_element_type=jnp.float32)
        before = carry[stacked_rows, :]
        weights = jnp.exp2(take + after + before)
        if diagonal:
            weights = jnp.where(key_place < query_place, weights, 0.0)
        acc[stacked_rows, :] += jnp.dot(weights.astype(jnp.bfloat16), values, preferred_element_type=jnp.float32)
        carry[stacked_rows, :] = before + (after[:, :1] + stay[:, :1])

    acc[...] = jnp.zeros_like(acc)
    carry[...] = jnp.zeros_like(carry)
    for key_tile in range(tiles - 1, -1, -1):
        span(kv_ref, key_tile, key_tile, key_tile + 1, True)
        if key_tile + 1 < tiles:
            span(kv_ref, key_tile, key_tile + 1, tiles, False)

    def receive(depth):
        place = (row - depth) * COLUMNS + col
        up_copy(held.at[place], depth - 1).wait_recv()

        @pl.when(row < rows - 1)
        def _():
            up_copy(held.at[place], depth).start()

        side_copy(held.at[place], depth).start()

    def step(index, unused):
        shard = me - 1 - index
        depth = row - shard // COLUMNS

        @pl.when(shard % COLUMNS != col)
        def _():
            @pl.when(depth + col <= row)
            def _():
                receive(depth + col)

            side_copy(held.at[shard], depth).wait_recv()

        source = held.at[shard]
        for key_tile in range(tiles - 1, -1, -1):
            span(source, key_tile, 0, tiles, False)
        return unused

    lax.fori_loop(0, me, step, 0)

    def finish(depth, unused):
        @pl.when(row < rows - 1)
        def _():
            up_copy(kv_ref, depth).wait_send()

        @pl.when((col == 0) | (depth > 0))
        def _():
            side_copy(kv_ref, depth).wait_send()

        return unused

    lax.fori_loop(0, row + 1, finish, 0)

    for query_tile in range(tiles):
        mixed = jnp.zeros((tile, width), jnp.float32)
        inverse = jnp.zeros((tile, width), jnp.float32)
        for head in range(heads):
            place = (query_tile * heads + head) * tile
            own = jnp.where(lane == head, acc[place : place + tile, :], 0.0)
            mean = jnp.sum(own * own, axis=1, keepdims=True) * (1.0 / HEAD_DIM)
            mixed = mixed + own
            inverse = jnp.where(lane == head, lax.rsqrt(mean + EPSILON), inverse)
        out_ref[query_tile * tile : (query_tile + 1) * tile, :] = (mixed * inverse * gain_ref[...]).astype(out_ref.dtype)


def attention(queries, key_heads, value_heads, head_gain):
    seq, width = queries.shape
    shards = lax.axis_size("sp")
    rows = shards // COLUMNS
    heads = width // HEAD_DIM
    both = jnp.concatenate([key_heads, value_heads], axis=1)
    vmem = pl.BlockSpec(memory_space=pltpu.VMEM)
    return pl.pallas_call(
        functools.partial(attention_kernel, rows),
        out_shape=jax.ShapeDtypeStruct((seq, width), jnp.bfloat16),
        in_specs=[vmem] * 3,
        out_specs=vmem,
        scratch_shapes=[
            pltpu.VMEM((shards, seq, 2 * width), jnp.bfloat16),
            pltpu.VMEM((heads * seq, width), jnp.bfloat16),
            pltpu.VMEM((heads * seq, width), jnp.float32),
            pltpu.VMEM((heads * seq, 1), jnp.float32),
            pltpu.SemaphoreType.DMA((rows,)),
            pltpu.SemaphoreType.DMA((rows,)),
            pltpu.SemaphoreType.DMA((rows,)),
            pltpu.SemaphoreType.DMA((rows,)),
        ],
        compiler_params=pltpu.CompilerParams(collective_id=0, has_side_effects=True),
        name="attention",
    )(queries, both, head_gain.reshape(1, width))


def round_up(value, unit):
    return (value + unit - 1) // unit * unit


def moe_kernel(
    rows, capacity, span, heads_ref, meta_ref, residual_ref, gain_ref, out_weight, shared_gate, shared_up, shared_down, expert_gate,
    expert_up, expert_down, out_ref, head_rows, meta_all, slots, place, mix, inputs, gathered, outgoing, arrived, returned, landed, base,
    gate_sum, up_sum, hidden, w_out, w_sgate, w_sup, w_sdown, w_gate, w_up, w_down, w_sem, head_send, head_recv, meta_send, meta_recv,
    up_send, up_recv, down_send, down_recv, go_send, go_recv, back_send, back_recv, part_send, part_recv):
    me = lax.axis_index("sp")
    tp = lax.axis_index("tp")
    row, col = me // COLUMNS, me % COLUMNS
    tp_size = head_rows.shape[0]
    group = COLUMNS * tp_size
    mine = col * tp_size + tp
    chunks, _, local, _, width = outgoing.shape
    count = residual_ref.shape[0]
    picks = meta_ref.shape[0] // 2
    total = group * local * span

    loads = []
    for index, (source, target) in enumerate((
            (out_weight, w_out), (expert_gate, w_gate), (expert_up, w_up), (expert_down, w_down),
            (shared_gate, w_sgate), (shared_up, w_sup), (shared_down, w_sdown))):
        loads.append(pltpu.make_async_copy(source, target, w_sem.at[index]))
        loads[-1].start()

    peers = []
    for across in range(COLUMNS - 1, -1, -1):
        for step in list(range(tp_size // 2, tp_size)) + list(range(tp_size // 2)):
            if across or step:
                peers.append(((col + across) % COLUMNS, (tp + step) % tp_size))

    def device(at_row, at_col, at_tp):
        return {"sp": at_row * COLUMNS + at_col, "tp": at_tp}

    barrier = pltpu.get_barrier_semaphore()
    for at_col, at_tp in peers:
        pl.semaphore_signal(barrier, inc=1, device_id=device(row, at_col, at_tp), device_id_type=MESH)
    for step in range(1, rows):
        pl.semaphore_signal(barrier, inc=1, device_id=device((row + step) % rows, col, tp), device_id_type=MESH)
    pl.semaphore_wait(barrier, len(peers) + rows - 1)

    def head_copy(to, source):
        return pltpu.make_async_remote_copy(
            src_ref=heads_ref.at[pl.ds(pl.multiple_of(to * count, count), count), :],
            dst_ref=head_rows.at[source], send_sem=head_send.at[to], recv_sem=head_recv.at[source],
            device_id=device(row, col, to), device_id_type=MESH)

    def meta_copy(to, source):
        return pltpu.make_async_remote_copy(
            src_ref=meta_ref, dst_ref=meta_all.at[source], send_sem=meta_send.at[to], recv_sem=meta_recv.at[source],
            device_id=device(to, col, tp), device_id_type=MESH)

    for step in range(1, tp_size):
        head_copy((tp + step) % tp_size, tp).start()
    for step in range(1, rows):
        meta_copy((row + step) % rows, row).start()
    head_rows[tp] = heads_ref[pl.ds(pl.multiple_of(tp * count, count), count), :]
    meta_all[row] = meta_ref[...]
    for step in range(1, rows):
        meta_copy((row + step) % rows, (row + step) % rows).wait_recv()

    expert_place = lax.broadcasted_iota(jnp.int32, (group * local, count), 0).astype(jnp.float32)
    slot_place = lax.broadcasted_iota(jnp.int32, (total, count), 0).astype(jnp.float32)
    first = lax.broadcasted_iota(jnp.int32, (count, count), 0)
    second = lax.broadcasted_iota(jnp.int32, (count, count), 1)
    earlier = (first < second).astype(jnp.bfloat16)
    lowest = (row * (group * local)).astype(jnp.float32)
    for block in range(rows):
        meta = meta_all[block]
        chosen = [meta[k : k + 1, :] - lowest for k in range(picks)]
        tables = [jnp.where(expert_place == chosen[k], 1.0, 0.0) for k in range(picks)]
        tally = jnp.dot(sum(tables).astype(jnp.bfloat16), earlier, preferred_element_type=jnp.float32)
        placed = jnp.zeros((total, count), jnp.float32)
        for k in range(picks):
            ranking = jnp.sum(tables[k] * tally, axis=0, keepdims=True)
            inside = (chosen[k] >= 0.0) & (chosen[k] < float(group * local))
            slot = jnp.where(inside, chosen[k] * float(span) + (block * capacity + ranking), -1.0)
            slots[block, k : k + 1, :] = slot
            placed = jnp.where(slot_place == slot, 1.0, placed)
        place[:, block * count : (block + 1) * count] = placed.astype(jnp.bfloat16)

    loads[0].wait()
    for step in range(1, tp_size):
        head_copy((tp + step) % tp_size, (tp + step) % tp_size).wait_recv()
    token_heads = jnp.concatenate([head_rows[source] for source in range(tp_size)], axis=1)
    branch = jnp.dot(token_heads, w_out[...], preferred_element_type=jnp.float32)
    stream = (residual_ref[...].astype(jnp.float32) + branch).astype(jnp.bfloat16).astype(jnp.float32)
    inverse = lax.rsqrt(jnp.mean(stream * stream, axis=1, keepdims=True) + EPSILON)
    normed = (stream * inverse * gain_ref[...]).astype(jnp.bfloat16)
    inputs[...] = normed
    for chunk in range(chunks):
        columns = slice(chunk * width, (chunk + 1) * width)
        base[chunk] = stream[:, columns]
        gathered[chunk, row] = normed[:, columns]

    def up_copy(chunk, block):
        return pltpu.make_async_remote_copy(
            src_ref=gathered.at[chunk, block], dst_ref=gathered.at[chunk, block], send_sem=up_send.at[chunk, block],
            recv_sem=up_recv.at[chunk, block], device_id=device(row + 1, col, tp), device_id_type=MESH)

    def down_copy(chunk, block):
        return pltpu.make_async_remote_copy(
            src_ref=gathered.at[chunk, block], dst_ref=gathered.at[chunk, block], send_sem=down_send.at[chunk, block],
            recv_sem=down_recv.at[chunk, block], device_id=device(row - 1, col, tp), device_id_type=MESH)

    def send_own(chunk):
        @pl.when(row < rows - 1)
        def _():
            up_copy(chunk, row).start()

        @pl.when(row > 0)
        def _():
            down_copy(chunk, row).start()

    def gather(chunk):
        for depth in range(1, rows):
            @pl.when(row >= depth)
            def _():
                up_copy(chunk, row - depth).wait_recv()

                @pl.when(row < rows - 1)
                def _():
                    up_copy(chunk, row - depth).start()

            @pl.when(row + depth < rows)
            def _():
                down_copy(chunk, row + depth).wait_recv()

                @pl.when(row > 0)
                def _():
                    down_copy(chunk, row + depth).start()

    def go_copy(chunk, peer, source):
        at_col, at_tp = peer
        return pltpu.make_async_remote_copy(
            src_ref=outgoing.at[chunk, at_col * tp_size + at_tp], dst_ref=arrived.at[chunk, :, source],
            send_sem=go_send.at[chunk, at_col * tp_size + at_tp], recv_sem=go_recv.at[chunk, source],
            device_id=device(row, at_col, at_tp), device_id_type=MESH)

    def back_copy(chunk, peer, source):
        at_col, at_tp = peer
        return pltpu.make_async_remote_copy(
            src_ref=outgoing.at[chunk, at_col * tp_size + at_tp], dst_ref=returned.at[chunk, source],
            send_sem=back_send.at[chunk, at_col * tp_size + at_tp], recv_sem=back_recv.at[chunk, source],
            device_id=device(row, at_col, at_tp), device_id_type=MESH)

    def part_copy(chunk, block, source):
        return pltpu.make_async_remote_copy(
            src_ref=gathered.at[chunk, block], dst_ref=landed.at[chunk, source], send_sem=part_send.at[chunk, block],
            recv_sem=part_recv.at[chunk, source], device_id=device(block, col, tp), device_id_type=MESH)

    def dispatch(chunk):
        tokens = gathered[chunk].reshape(rows * count, width)
        rows_out = jnp.dot(place[...], tokens, preferred_element_type=jnp.float32).astype(jnp.bfloat16)
        outgoing[chunk] = rows_out.reshape(group, local, span, width)
        arrived[chunk, :, mine] = outgoing[chunk, mine]
        for peer in peers:
            go_copy(chunk, peer, mine).start()

    def enter(chunk):
        for peer in peers:
            go_copy(chunk, peer, peer[0] * tp_size + peer[1]).wait_recv()
        deep = pl.ds(pl.multiple_of(chunk * width, width), width)
        for expert in range(local):
            block = arrived[chunk, expert].reshape(group * span, width)
            gate_sum[expert] += jnp.dot(block, w_gate[expert, deep, :], preferred_element_type=jnp.float32)
            up_sum[expert] += jnp.dot(block, w_up[expert, deep, :], preferred_element_type=jnp.float32)

    for chunk in range(min(2, chunks)):
        send_own(chunk)
    gate_sum[...] = jnp.zeros_like(gate_sum)
    up_sum[...] = jnp.zeros_like(up_sum)
    loads[1].wait()
    loads[2].wait()

    def forward(index, unused):
        @pl.when(index < chunks)
        def _():
            gather(index)

            @pl.when(index + 2 < chunks)
            def _():
                send_own(index + 2)

            dispatch(index)

        @pl.when(index >= LAG)
        def _():
            enter(index - LAG)

        return unused

    lax.fori_loop(0, chunks + LAG, forward, 0)

    for expert in range(local):
        gate = gate_sum[expert]
        hidden[expert] = (gate / (1.0 + jnp.exp(-gate)) * up_sum[expert]).astype(jnp.bfloat16)

    def sent(chunk, unused):
        for peer in peers:
            go_copy(chunk, peer, mine).wait_send()
        return unused

    lax.fori_loop(0, chunks, sent, 0)
    loads[3].wait()

    def leave(chunk, unused):
        wide = pl.ds(pl.multiple_of(chunk * width, width), width)
        for expert in range(local):
            down = jnp.dot(hidden[expert], w_down[expert, :, wide], preferred_element_type=jnp.float32).astype(jnp.bfloat16)
            outgoing[chunk, :, expert] = down.reshape(group, span, width)
        returned[chunk, mine] = outgoing[chunk, mine]
        for peer in peers:
            back_copy(chunk, peer, mine).start()
        return unused

    lax.fori_loop(0, chunks, leave, 0)

    for block in range(rows):
        weighed = jnp.zeros((total, count), jnp.float32)
        for k in range(picks):
            slot = slots[block, k : k + 1, :]
            weighed = jnp.where(slot_place == slot, meta_all[block, picks + k : picks + k + 1, :], weighed)
        mix[block] = weighed.T.astype(jnp.bfloat16)

    for load in loads[4:]:
        load.wait()

    def gathered_sent(chunk, unused):
        @pl.when(row < rows - 1)
        def _():
            def one(block, inner):
                up_copy(chunk, block).wait_send()
                return inner

            lax.fori_loop(0, row + 1, one, 0)

        @pl.when(row > 0)
        def _():
            def one(block, inner):
                down_copy(chunk, block).wait_send()
                return inner

            lax.fori_loop(row, rows, one, 0)

        return unused

    lax.fori_loop(0, chunks, gathered_sent, 0)
    x = inputs[...]
    shared = jnp.dot(x, w_sgate[...], preferred_element_type=jnp.float32)
    shared = (shared / (1.0 + jnp.exp(-shared)) * jnp.dot(x, w_sup[...], preferred_element_type=jnp.float32)).astype(jnp.bfloat16)
    for chunk in range(chunks):
        columns = slice(chunk * width, (chunk + 1) * width)
        base[chunk] += jnp.dot(shared, w_sdown[:, columns], preferred_element_type=jnp.float32)

    def combine(chunk, unused):
        for peer in peers:
            back_copy(chunk, peer, peer[0] * tp_size + peer[1]).wait_recv()
        results = returned[chunk].reshape(total, width)
        for step in range(1, rows):
            block = (row + step) % rows
            gathered[chunk, block] = jnp.dot(mix[block], results, preferred_element_type=jnp.float32).astype(jnp.bfloat16)
        base[chunk] += jnp.dot(mix[row], results, preferred_element_type=jnp.float32)
        for step in range(1, rows):
            part_copy(chunk, (row + step) % rows, row).start()
        return unused

    lax.fori_loop(0, chunks, combine, 0)

    def close(chunk, unused):
        value = base[chunk]
        for step in range(1, rows):
            source = (row + step) % rows
            part_copy(chunk, source, source).wait_recv()
            value += landed[chunk, source].astype(jnp.float32)
        out_ref[:, pl.ds(pl.multiple_of(chunk * width, width), width)] = value.astype(out_ref.dtype)
        for peer in peers:
            back_copy(chunk, peer, mine).wait_send()
        for step in range(1, rows):
            part_copy(chunk, (row + step) % rows, row).wait_send()
        return unused

    lax.fori_loop(0, chunks, close, 0)
    for step in range(1, tp_size):
        head_copy((tp + step) % tp_size, tp).wait_send()
    for step in range(1, rows):
        meta_copy((row + step) % rows, row).wait_send()


def experts(
    head_output, residual, out_weight, norm_gain, shared_gate, shared_up, shared_down, expert_gate, expert_up, expert_down,
    routed_experts, route_weights):
    count, picks = routed_experts.shape
    model = residual.shape[1]
    sp_size, tp_size = lax.axis_size("sp"), lax.axis_size("tp")
    rows, group = sp_size // COLUMNS, COLUMNS * tp_size
    local, _, inner = expert_gate.shape
    shared_inner = shared_gate.shape[1]
    expert_count = local * sp_size * tp_size
    capacity = max(2, 3 * count * picks // (2 * expert_count))
    span = round_up(rows * capacity, 16)
    total = group * local * span
    width = model // CHUNKS
    meta = jnp.concatenate([routed_experts.astype(jnp.float32).T, route_weights.T], axis=0)
    vmem = pl.BlockSpec(memory_space=pltpu.VMEM)
    hbm = pl.BlockSpec(memory_space=pl.ANY)
    half = jnp.bfloat16

    def pair(*shape):
        return [pltpu.SemaphoreType.DMA(shape)] * 2

    return pl.pallas_call(
        functools.partial(moe_kernel, rows, capacity, span),
        out_shape=jax.ShapeDtypeStruct((count, model), half),
        in_specs=[vmem] * 4 + [hbm] * 7,
        out_specs=vmem,
        scratch_shapes=[
            pltpu.VMEM((tp_size, count, head_output.shape[1]), half),
            pltpu.VMEM((rows, 2 * picks, count), jnp.float32),
            pltpu.VMEM((rows, 2 * picks, count), jnp.float32),
            pltpu.VMEM((total, rows * count), half),
            pltpu.VMEM((rows, count, total), half),
            pltpu.VMEM((count, model), half),
            pltpu.VMEM((CHUNKS, rows, count, width), half),
            pltpu.VMEM((CHUNKS, group, local, span, width), half),
            pltpu.VMEM((CHUNKS, local, group, span, width), half),
            pltpu.VMEM((CHUNKS, group, local, span, width), half),
            pltpu.VMEM((CHUNKS, rows, count, width), half),
            pltpu.VMEM((CHUNKS, count, width), jnp.float32),
            pltpu.VMEM((local, group * span, inner), jnp.float32),
            pltpu.VMEM((local, group * span, inner), jnp.float32),
            pltpu.VMEM((local, group * span, inner), half),
            pltpu.VMEM(out_weight.shape, half),
            pltpu.VMEM(shared_gate.shape, half),
            pltpu.VMEM(shared_up.shape, half),
            pltpu.VMEM(shared_down.shape, half),
            pltpu.VMEM(expert_gate.shape, half),
            pltpu.VMEM(expert_up.shape, half),
            pltpu.VMEM(expert_down.shape, half),
            pltpu.SemaphoreType.DMA((7,)),
            *pair(tp_size),
            *pair(rows),
            *pair(CHUNKS, rows),
            *pair(CHUNKS, rows),
            *pair(CHUNKS, group),
            *pair(CHUNKS, group),
            *pair(CHUNKS, rows),
        ],
        compiler_params=pltpu.CompilerParams(collective_id=1, has_side_effects=True, vmem_limit_bytes=VMEM_LIMIT),
        name="experts",
    )(head_output, meta, residual, norm_gain.reshape(1, model), out_weight, shared_gate, shared_up, shared_down,
      expert_gate, expert_up, expert_down)


def body(
    queries,
    key_heads,
    value_heads,
    head_gain,
    residual,
    out_weight,
    norm_gain,
    shared_gate,
    shared_up,
    shared_down,
    expert_gate,
    expert_up,
    expert_down,
    routed_experts,
    route_weights,
):
    head_output = attention(queries, key_heads, value_heads, head_gain)
    return experts(
        head_output, residual, out_weight, norm_gain, shared_gate, shared_up, shared_down, expert_gate, expert_up, expert_down,
        routed_experts, route_weights)


def solution(mesh):
    return jax.shard_map(
        body,
        mesh=mesh,
        in_specs=(
            P("sp", "tp"),
            P("sp", "tp"),
            P("sp", "tp"),
            P("tp"),
            P(("sp", "tp"), None),
            P(),
            P(),
            P(),
            P(),
            P(),
            P(("sp", "tp"), None, None),
            P(("sp", "tp"), None, None),
            P(("sp", "tp"), None, None),
            P(("sp", "tp"), None),
            P(("sp", "tp"), None),
        ),
        out_specs=P(("sp", "tp"), None),
        check_vma=False,
    )
```

```python
import functools
import math

import jax
import jax.numpy as jnp
from jax import lax
from jax.experimental import pallas as pl
from jax.experimental.pallas import tpu as pltpu
from jax.sharding import PartitionSpec as P

HEAD_DIM = 64


EPSILON = 1e-06

COLUMNS = 2
TILE = 256
LOG2E = 1.4426950408889634
MESH = pl.DeviceIdType.MESH
CHUNKS = 8
FIRST = 3
LAG = 2
PACK = 16
VMEM_LIMIT = 67043328


def attention_kernel(rows, q_ref, kv_ref, gain_ref, out_ref, held, masked, acc, carry, up_send, up_recv, side_send, side_recv):
    me = lax.axis_index("sp")
    row, col = me // COLUMNS, me % COLUMNS
    seq, width = q_ref.shape
    heads = width // HEAD_DIM
    tile = min(TILE, seq)
    tiles = seq // tile
    other = row * COLUMNS + (COLUMNS - 1 - col)

    barrier = pltpu.get_barrier_semaphore()

    @pl.when(row < rows - 1)
    def _():
        pl.semaphore_signal(barrier, inc=1, device_id={"sp": me + COLUMNS}, device_id_type=MESH)

    @pl.when(row > 0)
    def _():
        pl.semaphore_signal(barrier, inc=1, device_id={"sp": me - COLUMNS}, device_id_type=MESH)

    pl.semaphore_signal(barrier, inc=1, device_id={"sp": other}, device_id_type=MESH)
    inner = (row > 0) & (row < rows - 1)

    @pl.when(inner)
    def _():
        pl.semaphore_wait(barrier, 3)

    @pl.when(jnp.logical_not(inner))
    def _():
        pl.semaphore_wait(barrier, min(rows, 2))

    def up_copy(source, depth):
        place = (row - depth) * COLUMNS + col
        return pltpu.make_async_remote_copy(
            src_ref=source, dst_ref=held.at[place], send_sem=up_send.at[depth], recv_sem=up_recv.at[depth],
            device_id={"sp": me + COLUMNS}, device_id_type=MESH)

    def side_copy(source, depth):
        place = (row - depth) * COLUMNS + col
        return pltpu.make_async_remote_copy(
            src_ref=source, dst_ref=held.at[place], send_sem=side_send.at[depth], recv_sem=side_recv.at[depth],
            device_id={"sp": other}, device_id_type=MESH)

    @pl.when(row < rows - 1)
    def _():
        up_copy(kv_ref, 0).start()

    @pl.when(col == 0)
    def _():
        side_copy(kv_ref, 0).start()

    lane = lax.broadcasted_iota(jnp.int32, (1, width), 1) // HEAD_DIM
    key_row = lax.broadcasted_iota(jnp.int32, (tile, tile), 0)
    key_col = lax.broadcasted_iota(jnp.int32, (tile, tile), 1)
    later = (key_row > key_col).astype(jnp.bfloat16)
    scale = LOG2E / math.sqrt(HEAD_DIM)

    for head in range(heads):
        for query_tile in range(tiles):
            source_rows = slice(query_tile * tile, (query_tile + 1) * tile)
            stacked_rows = slice((query_tile * heads + head) * tile, (query_tile * heads + head + 1) * tile)
            masked[stacked_rows, :] = jnp.where(lane == head, q_ref[source_rows, :], jnp.zeros((), q_ref.dtype))

    def span(source, key_tile, first, last, diagonal):
        stacked_rows = slice(first * heads * tile, last * heads * tile)
        key_rows = slice(key_tile * tile, (key_tile + 1) * tile)
        keys = source[key_rows, :width]
        values = source[key_rows, width:]
        scores = lax.dot_general(masked[stacked_rows, :], keys, (((1,), (1,)), ((), ())), preferred_element_type=jnp.float32) * scale
        soft = jnp.log2(1.0 + jnp.exp2(-jnp.abs(scores)))
        take = jnp.minimum(scores, 0.0) - soft
        stay = take - scores
        if diagonal:
            query_place = jnp.concatenate([key_row] * ((last - first) * heads), axis=0)
            key_place = jnp.concatenate([key_col] * ((last - first) * heads), axis=0)
            stay = jnp.where(key_place < query_place, stay, 0.0)
        high = stay.astype(jnp.bfloat16)
        low = (stay - high.astype(jnp.float32)).astype(jnp.bfloat16)
        after = jnp.dot(high, later, preferred_element_type=jnp.float32) + jnp.dot(low, later, preferred_element_type=jnp.float32)
        before = carry[stacked_rows, :]
        weights = jnp.exp2(take + after + before)
        if diagonal:
            weights = jnp.where(key_place < query_place, weights, 0.0)
        acc[stacked_rows, :] += jnp.dot(weights.astype(jnp.bfloat16), values, preferred_element_type=jnp.float32)
        carry[stacked_rows, :] = before + (after[:, :1] + stay[:, :1])

    acc[...] = jnp.zeros_like(acc)
    carry[...] = jnp.zeros_like(carry)
    for key_tile in range(tiles - 1, -1, -1):
        span(kv_ref, key_tile, key_tile, key_tile + 1, True)
        if key_tile + 1 < tiles:
            span(kv_ref, key_tile, key_tile + 1, tiles, False)

    def receive(depth):
        place = (row - depth) * COLUMNS + col
        up_copy(held.at[place], depth - 1).wait_recv()

        @pl.when(row < rows - 1)
        def _():
            up_copy(held.at[place], depth).start()

        side_copy(held.at[place], depth).start()

    def step(index, unused):
        shard = me - 1 - index
        depth = row - shard // COLUMNS

        @pl.when(shard % COLUMNS != col)
        def _():
            @pl.when(depth + col <= row)
            def _():
                receive(depth + col)

            side_copy(held.at[shard], depth).wait_recv()

        source = held.at[shard]
        for key_tile in range(tiles - 1, -1, -1):
            span(source, key_tile, 0, tiles, False)
        return unused

    lax.fori_loop(0, me, step, 0)

    def finish(depth, unused):
        @pl.when(row < rows - 1)
        def _():
            up_copy(kv_ref, depth).wait_send()

        @pl.when((col == 0) | (depth > 0))
        def _():
            side_copy(kv_ref, depth).wait_send()

        return unused

    lax.fori_loop(0, row + 1, finish, 0)

    for query_tile in range(tiles):
        mixed = jnp.zeros((tile, width), jnp.float32)
        inverse = jnp.zeros((tile, width), jnp.float32)
        for head in range(heads):
            place = (query_tile * heads + head) * tile
            own = jnp.where(lane == head, acc[place : place + tile, :], 0.0)
            mean = jnp.sum(own * own, axis=1, keepdims=True) * (1.0 / HEAD_DIM)
            mixed = mixed + own
            inverse = jnp.where(lane == head, lax.rsqrt(mean + EPSILON), inverse)
        out_ref[query_tile * tile : (query_tile + 1) * tile, :] = (mixed * inverse * gain_ref[...]).astype(out_ref.dtype)


def attention(queries, key_heads, value_heads, head_gain):
    seq, width = queries.shape
    shards = lax.axis_size("sp")
    rows = shards // COLUMNS
    heads = width // HEAD_DIM
    both = jnp.concatenate([key_heads, value_heads], axis=1)
    vmem = pl.BlockSpec(memory_space=pltpu.VMEM)
    return pl.pallas_call(
        functools.partial(attention_kernel, rows),
        out_shape=jax.ShapeDtypeStruct((seq, width), jnp.bfloat16),
        in_specs=[vmem] * 3,
        out_specs=vmem,
        scratch_shapes=[
            pltpu.VMEM((shards, seq, 2 * width), jnp.bfloat16),
            pltpu.VMEM((heads * seq, width), jnp.bfloat16),
            pltpu.VMEM((heads * seq, width), jnp.float32),
            pltpu.VMEM((heads * seq, 1), jnp.float32),
            pltpu.SemaphoreType.DMA((rows,)),
            pltpu.SemaphoreType.DMA((rows,)),
            pltpu.SemaphoreType.DMA((rows,)),
            pltpu.SemaphoreType.DMA((rows,)),
        ],
        compiler_params=pltpu.CompilerParams(collective_id=0, has_side_effects=True),
        name="attention",
    )(queries, both, head_gain.reshape(1, width))


def round_up(value, unit):
    return (value + unit - 1) // unit * unit


def moe_kernel(
    rows, capacity, span, heads_ref, meta_ref, residual_ref, gain_ref, out_weight, shared_gate, shared_up, shared_down, expert_gate,
    expert_up, expert_down, out_ref, head_rows, meta_all, slots, place, mix, inputs, gathered, outgoing, arrived, returned, chained, landed,
    base, gate_sum, up_sum, hidden, w_out, w_sgate, w_sup, w_sdown, w_gate, w_up, w_down, w_sem, head_send, head_recv, meta_send,
    meta_recv, up_send, up_recv, down_send, down_recv, go_send, go_recv, back_send, back_recv, near_send, near_recv, chain_send,
    chain_recv, far_send, far_recv):
    me = lax.axis_index("sp")
    tp = lax.axis_index("tp")
    row, col = me // COLUMNS, me % COLUMNS
    tp_size = head_rows.shape[0]
    group = COLUMNS * tp_size
    mine = col * tp_size + tp
    _, chunks, _, block_rows, width = outgoing.shape
    local = gate_sum.shape[0]
    count = residual_ref.shape[0]
    picks = meta_ref.shape[0] // 2
    total = group * block_rows
    reach = rows // 2
    half = row // reach
    near_first, far_first = half * reach, (1 - half) * reach
    outward = (1 - half) * (reach - 1 - row) + half * (row - reach)
    inner_row = row + 1 - 2 * half
    bounds = [(e * span // PACK * PACK, round_up((e + 1) * span, PACK)) for e in range(local)]

    loads = []
    for index, (source, target) in enumerate((
            (out_weight, w_out), (expert_gate, w_gate), (expert_up, w_up), (expert_down, w_down),
            (shared_gate, w_sgate), (shared_up, w_sup), (shared_down, w_sdown))):
        loads.append(pltpu.make_async_copy(source, target, w_sem.at[index]))
        loads[-1].start()

    peers = []
    for across in range(COLUMNS - 1, -1, -1):
        for step in list(range(tp_size // 2, tp_size)) + list(range(tp_size // 2)):
            if across or step:
                peers.append(((col + across) % COLUMNS, (tp + step) % tp_size))

    def device(at_row, at_col, at_tp):
        return {"sp": at_row * COLUMNS + at_col, "tp": at_tp}

    barrier = pltpu.get_barrier_semaphore()
    for at_col, at_tp in peers:
        pl.semaphore_signal(barrier, inc=1, device_id=device(row, at_col, at_tp), device_id_type=MESH)
    for step in range(1, rows):
        pl.semaphore_signal(barrier, inc=1, device_id=device((row + step) % rows, col, tp), device_id_type=MESH)
    pl.semaphore_wait(barrier, len(peers) + rows - 1)

    def head_copy(to, source):
        return pltpu.make_async_remote_copy(
            src_ref=heads_ref.at[pl.ds(pl.multiple_of(to * count, count), count), :],
            dst_ref=head_rows.at[source], send_sem=head_send.at[to], recv_sem=head_recv.at[source],
            device_id=device(row, col, to), device_id_type=MESH)

    def meta_copy(to, source):
        return pltpu.make_async_remote_copy(
            src_ref=meta_ref, dst_ref=meta_all.at[source], send_sem=meta_send.at[to], recv_sem=meta_recv.at[source],
            device_id=device(to, col, tp), device_id_type=MESH)

    for step in range(1, tp_size):
        head_copy((tp + step) % tp_size, tp).start()
    for step in range(1, rows):
        meta_copy((row + step) % rows, row).start()
    head_rows[tp] = heads_ref[pl.ds(pl.multiple_of(tp * count, count), count), :]
    meta_all[row] = meta_ref[...]

    def up_copy(chunk, block):
        return pltpu.make_async_remote_copy(
            src_ref=gathered.at[chunk, block], dst_ref=gathered.at[chunk, block], send_sem=up_send.at[chunk, block],
            recv_sem=up_recv.at[chunk, block], device_id=device(row + 1, col, tp), device_id_type=MESH)

    def down_copy(chunk, block):
        return pltpu.make_async_remote_copy(
            src_ref=gathered.at[chunk, block], dst_ref=gathered.at[chunk, block], send_sem=down_send.at[chunk, block],
            recv_sem=down_recv.at[chunk, block], device_id=device(row - 1, col, tp), device_id_type=MESH)

    def from_below(chunk, block):
        up_copy(chunk, block).wait_recv()

        @pl.when(row < rows - 1)
        def _():
            up_copy(chunk, block).start()

    def from_above(chunk, block):
        down_copy(chunk, block).wait_recv()

        @pl.when(row > 0)
        def _():
            down_copy(chunk, block).start()

    def gather_near(chunk):
        for depth in range(1, reach):
            @pl.when(row - depth >= near_first)
            def _():
                from_below(chunk, row - depth)

            @pl.when(row + depth < near_first + reach)
            def _():
                from_above(chunk, row + depth)

    def gather_far(chunk):
        for depth in range(1, rows):
            @pl.when((row - depth >= 0) & (row - depth < near_first))
            def _():
                from_below(chunk, row - depth)

            @pl.when((row + depth >= near_first + reach) & (row + depth < rows))
            def _():
                from_above(chunk, row + depth)

    def go_copy(part, chunk, peer, source):
        at_col, at_tp = peer
        return pltpu.make_async_remote_copy(
            src_ref=outgoing.at[part, chunk, at_col * tp_size + at_tp], dst_ref=arrived.at[part, chunk, source],
            send_sem=go_send.at[part, chunk, at_col * tp_size + at_tp], recv_sem=go_recv.at[part, chunk, source],
            device_id=device(row, at_col, at_tp), device_id_type=MESH)

    def back_copy(part, chunk, peer, source):
        at_col, at_tp = peer
        return pltpu.make_async_remote_copy(
            src_ref=outgoing.at[part, chunk, at_col * tp_size + at_tp], dst_ref=returned.at[part, chunk, source],
            send_sem=back_send.at[part, chunk, at_col * tp_size + at_tp], recv_sem=back_recv.at[part, chunk, source],
            device_id=device(row, at_col, at_tp), device_id_type=MESH)

    def near_copy(chunk, block, source):
        return pltpu.make_async_remote_copy(
            src_ref=gathered.at[chunk, block], dst_ref=landed.at[chunk, source - near_first],
            send_sem=near_send.at[chunk, block - near_first], recv_sem=near_recv.at[chunk, source - near_first],
            device_id=device(block, col, tp), device_id_type=MESH)

    def chain_copy(chunk, index):
        return pltpu.make_async_remote_copy(
            src_ref=gathered.at[chunk, far_first + index], dst_ref=chained.at[chunk, index],
            send_sem=chain_send.at[chunk, index], recv_sem=chain_recv.at[chunk, index],
            device_id=device(inner_row, col, tp), device_id_type=MESH)

    def far_copy(chunk, index):
        return pltpu.make_async_remote_copy(
            src_ref=gathered.at[chunk, far_first + index], dst_ref=landed.at[chunk, reach],
            send_sem=far_send.at[chunk, index], recv_sem=far_recv.at[chunk],
            device_id=device(far_first + index, col, tp), device_id_type=MESH)

    def dispatch(part, chunk):
        first_block = near_first if part == 0 else far_first
        tokens = gathered[chunk, pl.ds(first_block, reach)].reshape(reach * count, width)
        rows_out = jnp.dot(place[part], tokens, preferred_element_type=jnp.float32).astype(jnp.bfloat16)
        outgoing[part, chunk] = rows_out.reshape(group, block_rows, width)
        arrived[part, chunk, mine] = outgoing[part, chunk, mine]
        for peer in peers:
            go_copy(part, chunk, peer, mine).start()

    def enter(part, chunk):
        for peer in peers:
            go_copy(part, chunk, peer, peer[0] * tp_size + peer[1]).wait_recv()
        deep = pl.ds(pl.multiple_of(chunk * width, width), width)
        for expert, (low, high) in enumerate(bounds):
            block = arrived[part, chunk, :, low:high, :].reshape(group * (high - low), width)
            gate_sum[expert] += jnp.dot(block, w_gate[expert, deep, :], preferred_element_type=jnp.float32)
            up_sum[expert] += jnp.dot(block, w_up[expert, deep, :], preferred_element_type=jnp.float32)

    def activate(part):
        for expert in range(local):
            gate = gate_sum[expert]
            hidden[part, expert] = (gate / (1.0 + jnp.exp(-gate)) * up_sum[expert]).astype(jnp.bfloat16)

    def leave(part, chunk):
        for peer in peers:
            go_copy(part, chunk, peer, mine).wait_send()
        wide = pl.ds(pl.multiple_of(chunk * width, width), width)
        downs = [
            jnp.dot(hidden[part, expert], w_down[expert, :, wide], preferred_element_type=jnp.float32).reshape(group, high - low, width)
            for expert, (low, high) in enumerate(bounds)]
        inside = lax.broadcasted_iota(jnp.int32, (1, PACK, 1), 1)
        for tile in range(0, block_rows, PACK):
            value = None
            for expert, (low, high) in enumerate(bounds):
                if low <= tile < high:
                    piece = downs[expert][:, tile - low : tile - low + PACK, :]
                    value = piece if value is None else jnp.where(inside + tile >= expert * span, piece, value)
            outgoing[part, chunk, :, tile : tile + PACK, :] = value.astype(jnp.bfloat16)
        returned[part, chunk, mine] = outgoing[part, chunk, mine]
        for peer in peers:
            back_copy(part, chunk, peer, mine).start()

    def combine(part, chunk):
        for peer in peers:
            back_copy(part, chunk, peer, peer[0] * tp_size + peer[1]).wait_recv()
        return returned[part, chunk].reshape(total, width)

    def combine_near(chunk):
        results = combine(0, chunk)
        for step in range(1, reach):
            block = near_first + (row - near_first + step) % reach
            gathered[chunk, block] = jnp.dot(mix[block], results, preferred_element_type=jnp.float32).astype(jnp.bfloat16)
        base[chunk] += jnp.dot(mix[row], results, preferred_element_type=jnp.float32)
        for step in range(1, reach):
            near_copy(chunk, near_first + (row - near_first + step) % reach, row).start()

    def combine_far(chunk):
        results = combine(1, chunk)
        for index in range(reach):
            block = far_first + index
            gathered[chunk, block] = jnp.dot(mix[block], results, preferred_element_type=jnp.float32).astype(jnp.bfloat16)

        @pl.when(outward == reach - 1)
        def _():
            onward(chunk)

    def onward(chunk):
        for index in range(reach):
            @pl.when(outward > 0)
            def _():
                chain_copy(chunk, index).start()

            @pl.when(outward == 0)
            def _():
                far_copy(chunk, index).start()

    def fold(chunk):
        @pl.when(outward < reach - 1)
        def _():
            for index in range(reach):
                chain_copy(chunk, index).wait_recv()
                block = far_first + index
                gathered[chunk, block] = (
                    gathered[chunk, block].astype(jnp.float32) + chained[chunk, index].astype(jnp.float32)).astype(jnp.bfloat16)
            onward(chunk)

    def loop(first, last, step):
        def one(index, unused):
            step(index)
            return unused

        lax.fori_loop(first, last, one, 0)

    for step in range(1, rows):
        meta_copy((row + step) % rows, (row + step) % rows).wait_recv()
    expert_place = lax.broadcasted_iota(jnp.int32, (group * local, count), 0).astype(jnp.float32)
    slot_place = lax.broadcasted_iota(jnp.int32, (total, count), 0).astype(jnp.float32)
    before = lax.broadcasted_iota(jnp.int32, (count, count), 0)
    after = lax.broadcasted_iota(jnp.int32, (count, count), 1)
    earlier = (before < after).astype(jnp.bfloat16)
    lowest = (row * (group * local)).astype(jnp.float32)
    for part in range(2):
        for index in range(reach):
            block = (near_first if part == 0 else far_first) + index
            meta = meta_all[block]
            chosen = [meta[k : k + 1, :] - lowest for k in range(picks)]
            tables = [jnp.where(expert_place == chosen[k], 1.0, 0.0) for k in range(picks)]
            tally = jnp.dot(sum(tables).astype(jnp.bfloat16), earlier, preferred_element_type=jnp.float32)
            placed = jnp.zeros((total, count), jnp.float32)
            for k in range(picks):
                ranking = jnp.sum(tables[k] * tally, axis=0, keepdims=True)
                inside = (chosen[k] >= 0.0) & (chosen[k] < float(group * local))
                owner = jnp.floor(chosen[k] * (1.0 / local))
                start = owner * float(block_rows) + (chosen[k] - owner * float(local)) * float(span)
                slot = jnp.where(inside, start + (index * capacity + ranking), -1.0)
                slots[block, k : k + 1, :] = slot
                placed = jnp.where(slot_place == slot, 1.0, placed)
            place[part, :, index * count : (index + 1) * count] = placed.astype(jnp.bfloat16)

    loads[0].wait()
    for step in range(1, tp_size):
        head_copy((tp + step) % tp_size, (tp + step) % tp_size).wait_recv()
    token_heads = jnp.concatenate([head_rows[source] for source in range(tp_size)], axis=1)
    branch = jnp.dot(token_heads, w_out[...], preferred_element_type=jnp.float32)
    stream = (residual_ref[...].astype(jnp.float32) + branch).astype(jnp.bfloat16).astype(jnp.float32)
    inverse = lax.rsqrt(jnp.mean(stream * stream, axis=1, keepdims=True) + EPSILON)
    normed = (stream * inverse * gain_ref[...]).astype(jnp.bfloat16)
    inputs[...] = normed
    for chunk in range(chunks):
        columns = slice(chunk * width, (chunk + 1) * width)
        base[chunk] = stream[:, columns]
        gathered[chunk, row] = normed[:, columns]

    def send_own(chunk):
        @pl.when(row < rows - 1)
        def _():
            up_copy(chunk, row).start()

        @pl.when(row > 0)
        def _():
            down_copy(chunk, row).start()

    loop(0, chunks, send_own)
    gate_sum[...] = jnp.zeros_like(gate_sum)
    up_sum[...] = jnp.zeros_like(up_sum)

    def near_step(chunk):
        gather_near(chunk)
        dispatch(0, chunk)

    loop(0, chunks, near_step)
    loads[1].wait()
    loads[2].wait()

    def far_step(chunk):
        gather_far(chunk)
        dispatch(1, chunk)
        enter(0, chunk)

    loop(0, chunks, far_step)
    activate(0)
    loads[3].wait()
    loop(0, FIRST, lambda chunk: leave(0, chunk))

    for load in loads[4:]:
        load.wait()
    x = inputs[...]
    shared = jnp.dot(x, w_sgate[...], preferred_element_type=jnp.float32)
    shared = (shared / (1.0 + jnp.exp(-shared)) * jnp.dot(x, w_sup[...], preferred_element_type=jnp.float32)).astype(jnp.bfloat16)
    for chunk in range(chunks):
        columns = slice(chunk * width, (chunk + 1) * width)
        base[chunk] += jnp.dot(shared, w_sdown[:, columns], preferred_element_type=jnp.float32)
    for block in range(rows):
        weighed = jnp.zeros((total, count), jnp.float32)
        for k in range(picks):
            slot = slots[block, k : k + 1, :]
            weighed = jnp.where(slot_place == slot, meta_all[block, picks + k : picks + k + 1, :], weighed)
        mix[block] = weighed.T.astype(jnp.bfloat16)

    gate_sum[...] = jnp.zeros_like(gate_sum)
    up_sum[...] = jnp.zeros_like(up_sum)
    loop(0, chunks, lambda chunk: enter(1, chunk))
    activate(1)
    loop(0, chunks, lambda chunk: leave(1, chunk))
    loop(FIRST, chunks, lambda chunk: leave(0, chunk))

    def gathered_sent(chunk):
        @pl.when(row < rows - 1)
        def _():
            loop(0, row + 1, lambda block: up_copy(chunk, block).wait_send())

        @pl.when(row > 0)
        def _():
            loop(row, rows, lambda block: down_copy(chunk, block).wait_send())

    loop(0, chunks, gathered_sent)
    loop(0, FIRST, combine_near)

    def far_back(index):
        combine_far(index)

        @pl.when(index >= LAG)
        def _():
            fold(index - LAG)

    loop(0, chunks, far_back)

    def near_back(index):
        combine_near(index)

        @pl.when(index - FIRST < LAG)
        def _():
            fold(index - FIRST + chunks - LAG)

    loop(FIRST, chunks, near_back)

    def close(chunk):
        value = base[chunk]
        far_copy(chunk, 0).wait_recv()
        value += landed[chunk, reach].astype(jnp.float32)
        for step in range(1, reach):
            source = near_first + (row - near_first + step) % reach
            near_copy(chunk, source, source).wait_recv()
            value += landed[chunk, source - near_first].astype(jnp.float32)
        out_ref[:, pl.ds(pl.multiple_of(chunk * width, width), width)] = value.astype(out_ref.dtype)

    loop(0, chunks, close)

    def settle(chunk):
        for peer in peers:
            back_copy(0, chunk, peer, mine).wait_send()
            back_copy(1, chunk, peer, mine).wait_send()
        for step in range(1, reach):
            near_copy(chunk, near_first + (row - near_first + step) % reach, row).wait_send()
        for index in range(reach):
            @pl.when(outward > 0)
            def _():
                chain_copy(chunk, index).wait_send()

            @pl.when(outward == 0)
            def _():
                far_copy(chunk, index).wait_send()

    loop(0, chunks, settle)
    for step in range(1, tp_size):
        head_copy((tp + step) % tp_size, tp).wait_send()
    for step in range(1, rows):
        meta_copy((row + step) % rows, row).wait_send()


def experts(
    head_output, residual, out_weight, norm_gain, shared_gate, shared_up, shared_down, expert_gate, expert_up, expert_down,
    routed_experts, route_weights):
    count, picks = routed_experts.shape
    model = residual.shape[1]
    sp_size, tp_size = lax.axis_size("sp"), lax.axis_size("tp")
    rows, group = sp_size // COLUMNS, COLUMNS * tp_size
    reach = rows // 2
    local, _, inner = expert_gate.shape
    expert_count = local * sp_size * tp_size
    capacity = max(2, 3 * count * picks // (2 * expert_count))
    span = round_up(reach * capacity, 8)
    block_rows = round_up(local * span, PACK)
    total = group * block_rows
    wide = max(round_up((e + 1) * span, PACK) - e * span // PACK * PACK for e in range(local))
    width = model // CHUNKS
    meta = jnp.concatenate([routed_experts.astype(jnp.float32).T, route_weights.T], axis=0)
    vmem = pl.BlockSpec(memory_space=pltpu.VMEM)
    hbm = pl.BlockSpec(memory_space=pl.ANY)
    half = jnp.bfloat16

    def pair(*shape):
        return [pltpu.SemaphoreType.DMA(shape)] * 2

    return pl.pallas_call(
        functools.partial(moe_kernel, rows, capacity, span),
        out_shape=jax.ShapeDtypeStruct((count, model), half),
        in_specs=[vmem] * 4 + [hbm] * 7,
        out_specs=vmem,
        scratch_shapes=[
            pltpu.VMEM((tp_size, count, head_output.shape[1]), half),
            pltpu.VMEM((rows, 2 * picks, count), jnp.float32),
            pltpu.VMEM((rows, 2 * picks, count), jnp.float32),
            pltpu.VMEM((2, total, reach * count), half),
            pltpu.VMEM((rows, count, total), half),
            pltpu.VMEM((count, model), half),
            pltpu.VMEM((CHUNKS, rows, count, width), half),
            pltpu.VMEM((2, CHUNKS, group, block_rows, width), half),
            pltpu.VMEM((2, CHUNKS, group, block_rows, width), half),
            pltpu.VMEM((2, CHUNKS, group, block_rows, width), half),
            pltpu.VMEM((CHUNKS, reach, count, width), half),
            pltpu.VMEM((CHUNKS, reach + 1, count, width), half),
            pltpu.VMEM((CHUNKS, count, width), jnp.float32),
            pltpu.VMEM((local, group * wide, inner), jnp.float32),
            pltpu.VMEM((local, group * wide, inner), jnp.float32),
            pltpu.VMEM((2, local, group * wide, inner), half),
            pltpu.VMEM(out_weight.shape, half),
            pltpu.VMEM(shared_gate.shape, half),
            pltpu.VMEM(shared_up.shape, half),
            pltpu.VMEM(shared_down.shape, half),
            pltpu.VMEM(expert_gate.shape, half),
            pltpu.VMEM(expert_up.shape, half),
            pltpu.VMEM(expert_down.shape, half),
            pltpu.SemaphoreType.DMA((7,)),
            *pair(tp_size),
            *pair(rows),
            *pair(CHUNKS, rows),
            *pair(CHUNKS, rows),
            *pair(2, CHUNKS, group),
            *pair(2, CHUNKS, group),
            *pair(CHUNKS, reach),
            *pair(CHUNKS, reach),
            pltpu.SemaphoreType.DMA((CHUNKS, reach)),
            pltpu.SemaphoreType.DMA((CHUNKS,)),
        ],
        compiler_params=pltpu.CompilerParams(collective_id=1, has_side_effects=True, vmem_limit_bytes=VMEM_LIMIT),
        name="experts",
    )(head_output, meta, residual, norm_gain.reshape(1, model), out_weight, shared_gate, shared_up, shared_down,
      expert_gate, expert_up, expert_down)


def body(
    queries,
    key_heads,
    value_heads,
    head_gain,
    residual,
    out_weight,
    norm_gain,
    shared_gate,
    shared_up,
    shared_down,
    expert_gate,
    expert_up,
    expert_down,
    routed_experts,
    route_weights,
):
    head_output = attention(queries, key_heads, value_heads, head_gain)
    return experts(
        head_output, residual, out_weight, norm_gain, shared_gate, shared_up, shared_down, expert_gate, expert_up, expert_down,
        routed_experts, route_weights)


def solution(mesh):
    return jax.shard_map(
        body,
        mesh=mesh,
        in_specs=(
            P("sp", "tp"),
            P("sp", "tp"),
            P("sp", "tp"),
            P("tp"),
            P(("sp", "tp"), None),
            P(),
            P(),
            P(),
            P(),
            P(),
            P(("sp", "tp"), None, None),
            P(("sp", "tp"), None, None),
            P(("sp", "tp"), None, None),
            P(("sp", "tp"), None),
            P(("sp", "tp"), None),
        ),
        out_specs=P(("sp", "tp"), None),
        check_vma=False,
    )
```

```python
import functools
import math

import jax
import jax.numpy as jnp
from jax import lax
from jax.experimental import pallas as pl
from jax.experimental.pallas import tpu as pltpu
from jax.sharding import PartitionSpec as P

HEAD_DIM = 64


EPSILON = 1e-06

COLUMNS = 2
TILE = 256
LOG2E = 1.4426950408889634
MESH = pl.DeviceIdType.MESH
CHUNKS = 8
FIRST = 2
LAG = 3
AHEAD = 3
PACK = 16
VMEM_LIMIT = 67043328


def attention_step(rows, q_ref, kv_ref, gain_ref, out_ref, held, masked, acc, carry, up_send, up_recv, side_send, side_recv):
    me = lax.axis_index("sp")
    row, col = me // COLUMNS, me % COLUMNS
    seq, width = q_ref.shape
    heads = width // HEAD_DIM
    tile = min(TILE, seq)
    tiles = seq // tile
    other = row * COLUMNS + (COLUMNS - 1 - col)

    def up_copy(source, depth, piece):
        place = (row - depth) * COLUMNS + col
        part = pl.ds(piece * tile, tile)
        return pltpu.make_async_remote_copy(
            src_ref=source.at[part, :], dst_ref=held.at[place, part, :], send_sem=up_send.at[depth, piece],
            recv_sem=up_recv.at[depth, piece], device_id={"sp": me + COLUMNS}, device_id_type=MESH)

    def side_copy(source, depth, piece):
        place = (row - depth) * COLUMNS + col
        part = pl.ds(piece * tile, tile)
        return pltpu.make_async_remote_copy(
            src_ref=source.at[part, :], dst_ref=held.at[place, part, :], send_sem=side_send.at[depth, piece],
            recv_sem=side_recv.at[depth, piece], device_id={"sp": other}, device_id_type=MESH)

    for piece in range(tiles - 1, -1, -1):
        @pl.when(row < rows - 1)
        def _():
            up_copy(kv_ref, 0, piece).start()

        @pl.when(col == 0)
        def _():
            side_copy(kv_ref, 0, piece).start()

    lane = lax.broadcasted_iota(jnp.int32, (1, width), 1) // HEAD_DIM
    key_row = lax.broadcasted_iota(jnp.int32, (tile, tile), 0)
    key_col = lax.broadcasted_iota(jnp.int32, (tile, tile), 1)
    later = (key_row > key_col).astype(jnp.bfloat16)
    scale = LOG2E / math.sqrt(HEAD_DIM)

    for head in range(heads):
        for query_tile in range(tiles):
            source_rows = slice(query_tile * tile, (query_tile + 1) * tile)
            stacked_rows = slice((query_tile * heads + head) * tile, (query_tile * heads + head + 1) * tile)
            masked[stacked_rows, :] = jnp.where(lane == head, q_ref[source_rows, :], jnp.zeros((), q_ref.dtype))

    def span(source, key_tile, first, last, diagonal):
        stacked_rows = slice(first * heads * tile, last * heads * tile)
        key_rows = slice(key_tile * tile, (key_tile + 1) * tile)
        keys = source[key_rows, :width]
        values = source[key_rows, width:]
        scores = lax.dot_general(masked[stacked_rows, :], keys, (((1,), (1,)), ((), ())), preferred_element_type=jnp.float32) * scale
        soft = lax.log(1.0 + jnp.exp2(-jnp.abs(scores))) * LOG2E
        take = jnp.minimum(scores, 0.0) - soft
        stay = take - scores
        if diagonal:
            query_place = jnp.concatenate([key_row] * ((last - first) * heads), axis=0)
            key_place = jnp.concatenate([key_col] * ((last - first) * heads), axis=0)
            stay = jnp.where(key_place < query_place, stay, 0.0)
        after = jnp.dot(stay.astype(jnp.bfloat16), later, preferred_element_type=jnp.float32)
        before = carry[stacked_rows, :]
        weights = jnp.exp2(take + after + before)
        if diagonal:
            weights = jnp.where(key_place < query_place, weights, 0.0)
        acc[stacked_rows, :] += jnp.dot(weights.astype(jnp.bfloat16), values, preferred_element_type=jnp.float32)
        carry[stacked_rows, :] = before + (after[:, :1] + stay[:, :1])

    acc[...] = jnp.zeros_like(acc)
    carry[...] = jnp.zeros_like(carry)
    for key_tile in range(tiles - 1, -1, -1):
        span(kv_ref, key_tile, key_tile, key_tile + 1, True)
        if key_tile + 1 < tiles:
            span(kv_ref, key_tile, key_tile + 1, tiles, False)

    def receive(depth, piece):
        place = (row - depth) * COLUMNS + col
        up_copy(held.at[place], depth - 1, piece).wait_recv()

        @pl.when(row < rows - 1)
        def _():
            up_copy(held.at[place], depth, piece).start()

        side_copy(held.at[place], depth, piece).start()

    def step(index, unused):
        shard = me - 1 - index
        depth = row - shard // COLUMNS

        @pl.when((index == 0) & (row > 0))
        def _():
            for key_tile in range(tiles - 1, -1, -1):
                receive(1, key_tile)

        source = held.at[shard]
        for key_tile in range(tiles - 1, -1, -1):
            @pl.when(shard % COLUMNS != col)
            def _():
                side_copy(held.at[shard], depth, key_tile).wait_recv()

            @pl.when((shard % COLUMNS == col) & (depth < row))
            def _():
                receive(depth + 1, key_tile)

            span(source, key_tile, 0, tiles, False)
        return unused

    lax.fori_loop(0, me, step, 0)

    def finish(depth, unused):
        @pl.when(row < rows - 1)
        def _():
            for piece in range(tiles):
                up_copy(kv_ref, depth, piece).wait_send()

        @pl.when((col == 0) | (depth > 0))
        def _():
            for piece in range(tiles):
                side_copy(kv_ref, depth, piece).wait_send()

        return unused

    lax.fori_loop(0, row + 1, finish, 0)

    for query_tile in range(tiles):
        mixed = jnp.zeros((tile, width), jnp.float32)
        inverse = jnp.zeros((tile, width), jnp.float32)
        for head in range(heads):
            place = (query_tile * heads + head) * tile
            own = jnp.where(lane == head, acc[place : place + tile, :], 0.0)
            mean = jnp.sum(own * own, axis=1, keepdims=True) * (1.0 / HEAD_DIM)
            mixed = mixed + own
            inverse = jnp.where(lane == head, lax.rsqrt(mean + EPSILON), inverse)
        out_ref[query_tile * tile : (query_tile + 1) * tile, :] = (mixed * inverse * gain_ref[...]).astype(out_ref.dtype)


def round_up(value, unit):
    return (value + unit - 1) // unit * unit


def layer_kernel(
    rows, capacity, span, q_ref, key_ref, value_ref, head_gain_ref, routed_ref, weight_ref, residual_ref, gain_ref, out_weight, shared_gate, shared_up, shared_down, expert_gate,
    expert_up, expert_down, out_ref, kv_ref, heads_ref, meta_ref, held, masked, acc, carry, q_up_send, q_up_recv, q_side_send, q_side_recv, head_rows, meta_all, slots, place, mix, gathered, parts, outgoing, arrived, returned, chained, landed,
    base, gate_sum, up_sum, hidden, w_out, w_sgate, w_sup, w_sdown, w_gate, w_up, w_down, w_sem, head_send, head_recv, meta_send,
    meta_recv, up_send, down_send, block_recv, go_send, go_recv, back_send, back_recv, near_send, near_recv, chain_send, chain_recv,
    far_send, far_recv):
    me = lax.axis_index("sp")
    tp = lax.axis_index("tp")
    row, col = me // COLUMNS, me % COLUMNS
    tp_size = head_rows.shape[0]
    group = COLUMNS * tp_size
    mine = col * tp_size + tp
    _, chunks, _, block_rows, width = outgoing.shape
    local = gate_sum.shape[0]
    count = residual_ref.shape[0]
    picks = routed_ref.shape[0]
    total = group * block_rows
    reach = rows // 2
    half = row // reach
    near_first, far_first = half * reach, (1 - half) * reach
    outward = (1 - half) * (reach - 1 - row) + half * (row - reach)
    inner_row = row + 1 - 2 * half
    bounds = [(e * span // PACK * PACK, round_up((e + 1) * span, PACK)) for e in range(local)]

    loads = []
    for index, (source, target) in enumerate((
            (out_weight, w_out), (shared_gate, w_sgate), (shared_up, w_sup), (shared_down, w_sdown),
            (expert_gate, w_gate), (expert_up, w_up), (expert_down, w_down))):
        loads.append(pltpu.make_async_copy(source, target, w_sem.at[index]))
        loads[-1].start()

    peers = []
    for across in range(COLUMNS - 1, -1, -1):
        for step in list(range(tp_size // 2, tp_size)) + list(range(tp_size // 2)):
            if across or step:
                peers.append(((col + across) % COLUMNS, (tp + step) % tp_size))

    def device(at_row, at_col, at_tp):
        return {"sp": at_row * COLUMNS + at_col, "tp": at_tp}

    def every(ref, semaphore):
        return pltpu.make_async_remote_copy(
            src_ref=ref, dst_ref=ref, send_sem=semaphore, recv_sem=semaphore, device_id=device(row, COLUMNS - 1 - col, tp),
            device_id_type=MESH)

    barrier = pltpu.get_barrier_semaphore()
    for at_col, at_tp in peers:
        pl.semaphore_signal(barrier, inc=1, device_id=device(row, at_col, at_tp), device_id_type=MESH)
    for step in range(1, rows):
        pl.semaphore_signal(barrier, inc=1, device_id=device((row + step) % rows, col, tp), device_id_type=MESH)
    pl.semaphore_wait(barrier, len(peers) + rows - 1)

    kv_ref[:, : key_ref.shape[1]] = key_ref[...]
    kv_ref[:, key_ref.shape[1] :] = value_ref[...]
    meta_ref[:picks, :] = routed_ref[...].astype(jnp.float32)
    meta_ref[picks:, :] = weight_ref[...]
    attention_step(
        rows, q_ref, kv_ref, head_gain_ref, heads_ref, held, masked, acc, carry, q_up_send, q_up_recv, q_side_send, q_side_recv)

    def head_copy(to, source):
        return pltpu.make_async_remote_copy(
            src_ref=heads_ref.at[pl.ds(pl.multiple_of(to * count, count), count), :],
            dst_ref=head_rows.at[source], send_sem=head_send, recv_sem=head_recv,
            device_id=device(row, col, to), device_id_type=MESH)

    def meta_copy(to, source):
        return pltpu.make_async_remote_copy(
            src_ref=meta_ref, dst_ref=meta_all.at[source], send_sem=meta_send, recv_sem=meta_recv,
            device_id=device(to, col, tp), device_id_type=MESH)

    for step in range(1, tp_size):
        head_copy((tp + step) % tp_size, tp).start()
    for step in range(1, rows):
        meta_copy((row + step) % rows, row).start()
    head_rows[tp] = heads_ref[pl.ds(pl.multiple_of(tp * count, count), count), :]
    meta_all[row] = meta_ref[...]

    def up_copy(chunk, block):
        return pltpu.make_async_remote_copy(
            src_ref=gathered.at[chunk, block], dst_ref=gathered.at[chunk, block], send_sem=up_send.at[block],
            recv_sem=block_recv.at[chunk, block], device_id=device(row + 1, col, tp), device_id_type=MESH)

    def down_copy(chunk, block):
        return pltpu.make_async_remote_copy(
            src_ref=gathered.at[chunk, block], dst_ref=gathered.at[chunk, block], send_sem=down_send.at[block],
            recv_sem=block_recv.at[chunk, block], device_id=device(row - 1, col, tp), device_id_type=MESH)

    def from_below(chunk, block):
        up_copy(chunk, block).wait_recv()

        @pl.when(row < rows - 1)
        def _():
            up_copy(chunk, block).start()

    def from_above(chunk, block):
        down_copy(chunk, block).wait_recv()

        @pl.when(row > 0)
        def _():
            down_copy(chunk, block).start()

    def gather_near(chunk):
        for depth in range(1, reach):
            @pl.when(row - depth >= near_first)
            def _():
                from_below(chunk, row - depth)

            @pl.when(row + depth < near_first + reach)
            def _():
                from_above(chunk, row + depth)

    def gather_far(chunk):
        for depth in range(1, rows):
            @pl.when((row - depth >= 0) & (row - depth < near_first))
            def _():
                from_below(chunk, row - depth)

            @pl.when((row + depth >= near_first + reach) & (row + depth < rows))
            def _():
                from_above(chunk, row + depth)

    def go_copy(part, chunk, peer, source):
        at_col, at_tp = peer
        return pltpu.make_async_remote_copy(
            src_ref=outgoing.at[part, chunk, at_col * tp_size + at_tp], dst_ref=arrived.at[part, chunk, source],
            send_sem=go_send.at[part], recv_sem=go_recv.at[part, chunk],
            device_id=device(row, at_col, at_tp), device_id_type=MESH)

    def back_copy(part, chunk, peer, source):
        at_col, at_tp = peer
        return pltpu.make_async_remote_copy(
            src_ref=outgoing.at[part, chunk, at_col * tp_size + at_tp], dst_ref=returned.at[part, chunk, source],
            send_sem=back_send, recv_sem=back_recv.at[part, chunk],
            device_id=device(row, at_col, at_tp), device_id_type=MESH)

    def near_copy(chunk, block, source):
        return pltpu.make_async_remote_copy(
            src_ref=parts.at[chunk, block], dst_ref=landed.at[chunk, source - near_first],
            send_sem=near_send, recv_sem=near_recv.at[chunk],
            device_id=device(block, col, tp), device_id_type=MESH)

    def chain_copy(chunk, index):
        return pltpu.make_async_remote_copy(
            src_ref=parts.at[chunk, far_first + index], dst_ref=chained.at[chunk, index],
            send_sem=chain_send, recv_sem=chain_recv.at[chunk],
            device_id=device(inner_row, col, tp), device_id_type=MESH)

    def far_copy(chunk, index):
        return pltpu.make_async_remote_copy(
            src_ref=parts.at[chunk, far_first + index], dst_ref=landed.at[chunk, reach],
            send_sem=far_send, recv_sem=far_recv.at[chunk],
            device_id=device(far_first + index, col, tp), device_id_type=MESH)

    def dispatch(part, chunk):
        first_block = near_first if part == 0 else far_first
        tokens = gathered[chunk, pl.ds(first_block, reach)].reshape(reach * count, width)
        rows_out = jnp.dot(place[part], tokens, preferred_element_type=jnp.float32).astype(jnp.bfloat16)
        outgoing[part, chunk] = rows_out.reshape(group, block_rows, width)
        arrived[part, chunk, mine] = outgoing[part, chunk, mine]
        for peer in peers:
            go_copy(part, chunk, peer, mine).start()

    def enter(part, chunk):
        every(arrived.at[part, chunk, pl.ds(0, group - 1)], go_recv.at[part, chunk]).wait_recv()
        deep = pl.ds(pl.multiple_of(chunk * width, width), width)
        for expert, (low, high) in enumerate(bounds):
            block = arrived[part, chunk, :, low:high, :].reshape(group * (high - low), width)
            gate_sum[expert] += jnp.dot(block, w_gate[expert, deep, :], preferred_element_type=jnp.float32)
            up_sum[expert] += jnp.dot(block, w_up[expert, deep, :], preferred_element_type=jnp.float32)

    def activate(part):
        for expert in range(local):
            gate = gate_sum[expert]
            hidden[part, expert] = (gate / (1.0 + jnp.exp(-gate)) * up_sum[expert]).astype(jnp.bfloat16)

    def leave(part, chunk):
        wide = pl.ds(pl.multiple_of(chunk * width, width), width)
        downs = [
            jnp.dot(hidden[part, expert], w_down[expert, :, wide], preferred_element_type=jnp.float32).reshape(group, high - low, width)
            for expert, (low, high) in enumerate(bounds)]
        inside = lax.broadcasted_iota(jnp.int32, (1, PACK, 1), 1)
        for tile in range(0, block_rows, PACK):
            value = None
            for expert, (low, high) in enumerate(bounds):
                if low <= tile < high:
                    piece = downs[expert][:, tile - low : tile - low + PACK, :]
                    value = piece if value is None else jnp.where(inside + tile >= expert * span, piece, value)
            outgoing[part, chunk, :, tile : tile + PACK, :] = value.astype(jnp.bfloat16)
        returned[part, chunk, mine] = outgoing[part, chunk, mine]
        for peer in peers:
            back_copy(part, chunk, peer, mine).start()

    def combine(part, chunk):
        every(returned.at[part, chunk, pl.ds(0, group - 1)], back_recv.at[part, chunk]).wait_recv()
        return returned[part, chunk].reshape(total, width)

    def combine_near(chunk):
        results = combine(0, chunk)
        for step in range(1, reach):
            block = near_first + (row - near_first + step) % reach
            parts[chunk, block] = jnp.dot(mix[block], results, preferred_element_type=jnp.float32).astype(jnp.bfloat16)
        base[chunk] += jnp.dot(mix[row], results, preferred_element_type=jnp.float32)
        for step in range(1, reach):
            near_copy(chunk, near_first + (row - near_first + step) % reach, row).start()

    def combine_far(chunk):
        results = combine(1, chunk)
        for index in range(reach):
            block = far_first + index
            parts[chunk, block] = jnp.dot(mix[block], results, preferred_element_type=jnp.float32).astype(jnp.bfloat16)

        @pl.when(outward == reach - 1)
        def _():
            onward(chunk)

    def onward(chunk):
        for index in range(reach):
            @pl.when(outward > 0)
            def _():
                chain_copy(chunk, index).start()

            @pl.when(outward == 0)
            def _():
                far_copy(chunk, index).start()

    def fold(chunk):
        @pl.when(outward < reach - 1)
        def _():
            every(chained.at[chunk], chain_recv.at[chunk]).wait_recv()
            for index in range(reach):
                block = far_first + index
                parts[chunk, block] = (
                    parts[chunk, block].astype(jnp.float32) + chained[chunk, index].astype(jnp.float32)).astype(jnp.bfloat16)
            onward(chunk)

    def loop(first, last, step):
        def one(index, unused):
            step(index)
            return unused

        lax.fori_loop(first, last, one, 0)

    loads[0].wait()
    every(head_rows.at[pl.ds(0, tp_size - 1)], head_recv).wait_recv()
    token_heads = jnp.concatenate([head_rows[source] for source in range(tp_size)], axis=1)
    branch = jnp.dot(token_heads, w_out[...], preferred_element_type=jnp.float32)
    stream = (residual_ref[...].astype(jnp.float32) + branch).astype(jnp.bfloat16).astype(jnp.float32)
    inverse = lax.rsqrt(jnp.mean(stream * stream, axis=1, keepdims=True) + EPSILON)
    normed = (stream * inverse * gain_ref[...]).astype(jnp.bfloat16)
    for chunk in range(chunks):
        columns = slice(chunk * width, (chunk + 1) * width)
        base[chunk] = stream[:, columns]
        gathered[chunk, row] = normed[:, columns]

    def send_own(chunk):
        @pl.when(row < rows - 1)
        def _():
            up_copy(chunk, row).start()

        @pl.when(row > 0)
        def _():
            down_copy(chunk, row).start()

    loop(0, chunks, send_own)
    every(meta_all.at[pl.ds(0, rows - 1)], meta_recv).wait_recv()
    expert_place = lax.broadcasted_iota(jnp.int32, (group * local, count), 0).astype(jnp.float32)
    slot_place = lax.broadcasted_iota(jnp.int32, (total, count), 0).astype(jnp.float32)
    before = lax.broadcasted_iota(jnp.int32, (count, count), 0)
    after = lax.broadcasted_iota(jnp.int32, (count, count), 1)
    earlier = (before < after).astype(jnp.bfloat16)
    lowest = (row * (group * local)).astype(jnp.float32)
    for part in range(2):
        for index in range(reach):
            block = (near_first if part == 0 else far_first) + index
            meta = meta_all[block]
            chosen = [meta[k : k + 1, :] - lowest for k in range(picks)]
            tables = [jnp.where(expert_place == chosen[k], 1.0, 0.0) for k in range(picks)]
            tally = jnp.dot(sum(tables).astype(jnp.bfloat16), earlier, preferred_element_type=jnp.float32)
            placed = jnp.zeros((total, count), jnp.float32)
            for k in range(picks):
                ranking = jnp.sum(tables[k] * tally, axis=0, keepdims=True)
                inside = (chosen[k] >= 0.0) & (chosen[k] < float(group * local))
                owner = jnp.floor(chosen[k] * (1.0 / local))
                start = owner * float(block_rows) + (chosen[k] - owner * float(local)) * float(span)
                slot = jnp.where(inside, start + (index * capacity + ranking), -1.0)
                slots[block, k : k + 1, :] = slot
                placed = jnp.where(slot_place == slot, 1.0, placed)
            place[part, :, index * count : (index + 1) * count] = placed.astype(jnp.bfloat16)

    for block in range(rows):
        weighed = jnp.zeros((total, count), jnp.float32)
        for k in range(picks):
            slot = slots[block, k : k + 1, :]
            weighed = jnp.where(slot_place == slot, meta_all[block, picks + k : picks + k + 1, :], weighed)
        mix[block] = weighed.T.astype(jnp.bfloat16)

    gate_sum[...] = jnp.zeros_like(gate_sum)
    up_sum[...] = jnp.zeros_like(up_sum)
    for load in loads[1:4]:
        load.wait()
    shared = jnp.dot(normed, w_sgate[...], preferred_element_type=jnp.float32)
    shared = shared / (1.0 + jnp.exp(-shared)) * jnp.dot(normed, w_sup[...], preferred_element_type=jnp.float32)
    shared = shared.astype(jnp.bfloat16)
    for chunk in range(chunks):
        columns = slice(chunk * width, (chunk + 1) * width)
        base[chunk] += jnp.dot(shared, w_sdown[:, columns], preferred_element_type=jnp.float32)

    def near_step(chunk):
        gather_near(chunk)
        dispatch(0, chunk)

    loop(0, chunks, near_step)
    for load in loads[4:]:
        load.wait()

    split = chunks // 2

    def far_step(chunk):
        gather_far(chunk)
        dispatch(1, chunk)

        @pl.when(chunk < split)
        def _():
            enter(0, 2 * chunk)
            enter(0, 2 * chunk + 1)

        @pl.when(chunk == split)
        def _():
            activate(0)
            gate_sum[...] = jnp.zeros_like(gate_sum)
            up_sum[...] = jnp.zeros_like(up_sum)

        @pl.when(chunk >= split)
        def _():
            enter(1, chunk - split)

    loop(0, chunks, far_step)
    every(outgoing.at[0, :, pl.ds(0, group - 1)], go_send.at[0]).wait_send()
    loop(0, FIRST, lambda chunk: leave(0, chunk))
    loop(chunks - split, chunks, lambda chunk: enter(1, chunk))
    activate(1)
    every(outgoing.at[1, :, pl.ds(0, group - 1)], go_send.at[1]).wait_send()

    loop(0, AHEAD, lambda chunk: leave(1, chunk))

    def far_back(index):
        @pl.when(index + AHEAD < chunks)
        def _():
            leave(1, index + AHEAD)

        @pl.when(index + AHEAD >= chunks)
        def _():
            leave(0, index + AHEAD - chunks + FIRST)

        @pl.when(index < FIRST)
        def _():
            combine_near(index)

        combine_far(index)

        @pl.when(index >= LAG)
        def _():
            fold(index - LAG)

    loop(0, chunks, far_back)

    def close(chunk):
        value = base[chunk]
        far_copy(chunk, 0).wait_recv()
        value += landed[chunk, reach].astype(jnp.float32)
        every(landed.at[chunk, pl.ds(0, reach - 1)], near_recv.at[chunk]).wait_recv()
        for step in range(1, reach):
            source = near_first + (row - near_first + step) % reach
            value += landed[chunk, source - near_first].astype(jnp.float32)
        out_ref[:, pl.ds(pl.multiple_of(chunk * width, width), width)] = value.astype(out_ref.dtype)

    def near_back(index):
        @pl.when(index + AHEAD < chunks)
        def _():
            leave(0, index + AHEAD)

        combine_near(index)
        turn = index - FIRST

        @pl.when((turn >= 1) & (turn <= LAG))
        def _():
            fold(chunks - LAG + turn - 1)

        @pl.when(turn >= LAG)
        def _():
            close(turn - LAG)

    loop(FIRST, chunks, near_back)
    loop(chunks - FIRST - LAG, chunks, close)
    every(outgoing.at[:, :, pl.ds(0, group - 1)], back_send).wait_send()
    every(parts.at[:, pl.ds(0, reach - 1)], near_send).wait_send()

    @pl.when(outward > 0)
    def _():
        every(parts.at[:, pl.ds(0, reach)], chain_send).wait_send()

    @pl.when(outward == 0)
    def _():
        every(parts.at[:, pl.ds(0, reach)], far_send).wait_send()

    @pl.when(row < rows - 1)
    def _():
        loop(0, row + 1, lambda block: every(gathered.at[:, block], up_send.at[block]).wait_send())

    @pl.when(row > 0)
    def _():
        loop(row, rows, lambda block: every(gathered.at[:, block], down_send.at[block]).wait_send())

    every(head_rows.at[pl.ds(0, tp_size - 1)], head_send).wait_send()
    every(meta_all.at[pl.ds(0, rows - 1)], meta_send).wait_send()


def layer(
    queries, key_heads, value_heads, head_gain, residual, out_weight, norm_gain, shared_gate, shared_up, shared_down, expert_gate, expert_up, expert_down,
    routed_experts, route_weights):
    count, picks = routed_experts.shape
    model = residual.shape[1]
    sp_size, tp_size = lax.axis_size("sp"), lax.axis_size("tp")
    rows, group = sp_size // COLUMNS, COLUMNS * tp_size
    reach = rows // 2
    local, _, inner = expert_gate.shape
    expert_count = local * sp_size * tp_size
    capacity = max(2, 3 * count * picks // (2 * expert_count))
    span = round_up(reach * capacity, 8)
    block_rows = round_up(local * span, PACK)
    total = group * block_rows
    wide = max(round_up((e + 1) * span, PACK) - e * span // PACK * PACK for e in range(local))
    width = model // CHUNKS
    seq, head_width = queries.shape
    heads = head_width // HEAD_DIM
    pieces = -(-seq // TILE)
    vmem = pl.BlockSpec(memory_space=pltpu.VMEM)
    hbm = pl.BlockSpec(memory_space=pl.ANY)
    half = jnp.bfloat16

    return pl.pallas_call(
        functools.partial(layer_kernel, rows, capacity, span),
        out_shape=jax.ShapeDtypeStruct((count, model), half),
        in_specs=[vmem] * 8 + [hbm] * 7,
        out_specs=vmem,
        scratch_shapes=[
            pltpu.VMEM((seq, 2 * head_width), half),
            pltpu.VMEM((seq, head_width), half),
            pltpu.VMEM((2 * picks, count), jnp.float32),
            pltpu.VMEM((sp_size, seq, 2 * head_width), half),
            pltpu.VMEM((heads * seq, head_width), half),
            pltpu.VMEM((heads * seq, head_width), jnp.float32),
            pltpu.VMEM((heads * seq, 1), jnp.float32),
            *[pltpu.SemaphoreType.DMA((rows, pieces))] * 4,
            pltpu.VMEM((tp_size, count, head_width), half),
            pltpu.VMEM((rows, 2 * picks, count), jnp.float32),
            pltpu.VMEM((rows, 2 * picks, count), jnp.float32),
            pltpu.VMEM((2, total, reach * count), half),
            pltpu.VMEM((rows, count, total), half),
            pltpu.VMEM((CHUNKS, rows, count, width), half),
            pltpu.VMEM((CHUNKS, rows, count, width), half),
            pltpu.VMEM((2, CHUNKS, group, block_rows, width), half),
            pltpu.VMEM((2, CHUNKS, group, block_rows, width), half),
            pltpu.VMEM((2, CHUNKS, group, block_rows, width), half),
            pltpu.VMEM((CHUNKS, reach, count, width), half),
            pltpu.VMEM((CHUNKS, reach + 1, count, width), half),
            pltpu.VMEM((CHUNKS, count, width), jnp.float32),
            pltpu.VMEM((local, group * wide, inner), jnp.float32),
            pltpu.VMEM((local, group * wide, inner), jnp.float32),
            pltpu.VMEM((2, local, group * wide, inner), half),
            pltpu.VMEM(out_weight.shape, half),
            pltpu.VMEM(shared_gate.shape, half),
            pltpu.VMEM(shared_up.shape, half),
            pltpu.VMEM(shared_down.shape, half),
            pltpu.VMEM(expert_gate.shape, half),
            pltpu.VMEM(expert_up.shape, half),
            pltpu.VMEM(expert_down.shape, half),
            pltpu.SemaphoreType.DMA((7,)),
            *[pltpu.SemaphoreType.DMA] * 4,
            *[pltpu.SemaphoreType.DMA((rows,))] * 2,
            pltpu.SemaphoreType.DMA((CHUNKS, rows)),
            pltpu.SemaphoreType.DMA((2,)),
            pltpu.SemaphoreType.DMA((2, CHUNKS)),
            pltpu.SemaphoreType.DMA,
            pltpu.SemaphoreType.DMA((2, CHUNKS)),
            *[pltpu.SemaphoreType.DMA, pltpu.SemaphoreType.DMA((CHUNKS,))] * 3,
        ],
        compiler_params=pltpu.CompilerParams(collective_id=0, has_side_effects=True, vmem_limit_bytes=VMEM_LIMIT),
        name="layer",
    )(queries, key_heads, value_heads, head_gain.reshape(1, head_width), routed_experts.T, route_weights.T, residual, norm_gain.reshape(1, model), out_weight, shared_gate, shared_up, shared_down,
      expert_gate, expert_up, expert_down)


def body(
    queries,
    key_heads,
    value_heads,
    head_gain,
    residual,
    out_weight,
    norm_gain,
    shared_gate,
    shared_up,
    shared_down,
    expert_gate,
    expert_up,
    expert_down,
    routed_experts,
    route_weights,
):
    return layer(
        queries, key_heads, value_heads, head_gain, residual, out_weight, norm_gain, shared_gate, shared_up, shared_down,
        expert_gate, expert_up, expert_down, routed_experts, route_weights)


def solution(mesh):
    return jax.shard_map(
        body,
        mesh=mesh,
        in_specs=(
            P("sp", "tp"),
            P("sp", "tp"),
            P("sp", "tp"),
            P("tp"),
            P(("sp", "tp"), None),
            P(),
            P(),
            P(),
            P(),
            P(),
            P(("sp", "tp"), None, None),
            P(("sp", "tp"), None, None),
            P(("sp", "tp"), None, None),
            P(("sp", "tp"), None),
            P(("sp", "tp"), None),
        ),
        out_specs=P(("sp", "tp"), None),
        check_vma=False,
    )
```

```python
import functools
import math

import jax
import jax.numpy as jnp
from jax import lax
from jax.experimental import pallas as pl
from jax.experimental.pallas import tpu as pltpu
from jax.sharding import PartitionSpec as P

HEAD_DIM = 64


EPSILON = 1e-06

COLUMNS = 2
TILE = 256
LOG2E = 1.4426950408889634
MESH = pl.DeviceIdType.MESH
CHUNKS = 8
FIRST = 2
LAG = 3
AHEAD = 3
SPLIT = 2
PACK = 16
VMEM_LIMIT = 67043328


def attention_step(rows, q_ref, kv_ref, gain_ref, out_ref, held, masked, acc, carry, up_send, up_recv, side_send, side_recv):
    me = lax.axis_index("sp")
    row, col = me // COLUMNS, me % COLUMNS
    seq, width = q_ref.shape
    heads = width // HEAD_DIM
    tile = min(TILE, seq)
    tiles = seq // tile
    other = row * COLUMNS + (COLUMNS - 1 - col)

    short = tile // SPLIT

    def up_copy(source, depth, piece):
        place = (row - depth) * COLUMNS + col
        part = pl.ds(piece * short, short)
        return pltpu.make_async_remote_copy(
            src_ref=source.at[part, :], dst_ref=held.at[place, part, :], send_sem=up_send.at[depth],
            recv_sem=up_recv.at[depth, piece], device_id={"sp": me + COLUMNS}, device_id_type=MESH)

    def side_copy(source, depth, piece):
        place = (row - depth) * COLUMNS + col
        part = pl.ds(piece * short, short)
        return pltpu.make_async_remote_copy(
            src_ref=source.at[part, :], dst_ref=held.at[place, part, :], send_sem=side_send.at[depth],
            recv_sem=side_recv.at[depth, piece], device_id={"sp": other}, device_id_type=MESH)

    def whole_copy(semaphore):
        return pltpu.make_async_remote_copy(
            src_ref=kv_ref, dst_ref=kv_ref, send_sem=semaphore, recv_sem=semaphore, device_id={"sp": other}, device_id_type=MESH)

    for piece in range(tiles * SPLIT - 1, -1, -1):
        @pl.when(row < rows - 1)
        def _():
            up_copy(kv_ref, 0, piece).start()

        @pl.when(col == 0)
        def _():
            side_copy(kv_ref, 0, piece).start()

    lane = lax.broadcasted_iota(jnp.int32, (1, width), 1) // HEAD_DIM
    key_row = lax.broadcasted_iota(jnp.int32, (tile, tile), 0)
    key_col = lax.broadcasted_iota(jnp.int32, (tile, tile), 1)
    later = (key_row > key_col).astype(jnp.bfloat16)
    scale = LOG2E / math.sqrt(HEAD_DIM)

    for head in range(heads):
        for query_tile in range(tiles):
            source_rows = slice(query_tile * tile, (query_tile + 1) * tile)
            stacked_rows = slice((query_tile * heads + head) * tile, (query_tile * heads + head + 1) * tile)
            masked[stacked_rows, :] = jnp.where(lane == head, q_ref[source_rows, :], jnp.zeros((), q_ref.dtype))

    def span(source, key_tile, first, last, diagonal):
        stacked_rows = slice(first * heads * tile, last * heads * tile)
        key_rows = slice(key_tile * tile, (key_tile + 1) * tile)
        keys = source[key_rows, :width]
        values = source[key_rows, width:]
        scores = lax.dot_general(masked[stacked_rows, :], keys, (((1,), (1,)), ((), ())), preferred_element_type=jnp.float32) * scale
        soft = lax.log(1.0 + jnp.exp2(-jnp.abs(scores))) * LOG2E
        take = jnp.minimum(scores, 0.0) - soft
        stay = take - scores
        if diagonal:
            query_place = jnp.concatenate([key_row] * ((last - first) * heads), axis=0)
            key_place = jnp.concatenate([key_col] * ((last - first) * heads), axis=0)
            stay = jnp.where(key_place < query_place, stay, 0.0)
        after = jnp.dot(stay.astype(jnp.bfloat16), later, preferred_element_type=jnp.float32)
        before = carry[stacked_rows, :]
        weights = jnp.exp2(take + after + before)
        if diagonal:
            weights = jnp.where(key_place < query_place, weights, 0.0)
        acc[stacked_rows, :] += jnp.dot(weights.astype(jnp.bfloat16), values, preferred_element_type=jnp.float32)
        carry[stacked_rows, :] = before + (after[:, :1] + stay[:, :1])

    acc[...] = jnp.zeros_like(acc)
    carry[...] = jnp.zeros_like(carry)
    for key_tile in range(tiles - 1, -1, -1):
        span(kv_ref, key_tile, key_tile, key_tile + 1, True)
        if key_tile + 1 < tiles:
            span(kv_ref, key_tile, key_tile + 1, tiles, False)

    def receive(depth, key_tile):
        place = (row - depth) * COLUMNS + col
        for piece in range((key_tile + 1) * SPLIT - 1, key_tile * SPLIT - 1, -1):
            up_copy(held.at[place], depth - 1, piece).wait_recv()

            @pl.when(row < rows - 1)
            def _():
                up_copy(held.at[place], depth, piece).start()

            side_copy(held.at[place], depth, piece).start()

    def step(index, unused):
        shard = me - 1 - index
        depth = row - shard // COLUMNS

        @pl.when((index == 0) & (row > 0))
        def _():
            for key_tile in range(tiles - 1, -1, -1):
                receive(1, key_tile)

        source = held.at[shard]
        for key_tile in range(tiles - 1, -1, -1):
            @pl.when(shard % COLUMNS != col)
            def _():
                for piece in range((key_tile + 1) * SPLIT - 1, key_tile * SPLIT - 1, -1):
                    side_copy(held.at[shard], depth, piece).wait_recv()

            @pl.when((shard % COLUMNS == col) & (depth < row))
            def _():
                receive(depth + 1, key_tile)

            span(source, key_tile, 0, tiles, False)
        return unused

    lax.fori_loop(0, me, step, 0)

    def finish(depth, unused):
        @pl.when(row < rows - 1)
        def _():
            whole_copy(up_send.at[depth]).wait_send()

        @pl.when((col == 0) | (depth > 0))
        def _():
            whole_copy(side_send.at[depth]).wait_send()

        return unused

    lax.fori_loop(0, row + 1, finish, 0)

    for query_tile in range(tiles):
        mixed = jnp.zeros((tile, width), jnp.float32)
        inverse = jnp.zeros((tile, width), jnp.float32)
        for head in range(heads):
            place = (query_tile * heads + head) * tile
            own = jnp.where(lane == head, acc[place : place + tile, :], 0.0)
            mean = jnp.sum(own * own, axis=1, keepdims=True) * (1.0 / HEAD_DIM)
            mixed = mixed + own
            inverse = jnp.where(lane == head, lax.rsqrt(mean + EPSILON), inverse)
        out_ref[query_tile * tile : (query_tile + 1) * tile, :] = (mixed * inverse * gain_ref[...]).astype(out_ref.dtype)


def round_up(value, unit):
    return (value + unit - 1) // unit * unit


def layer_kernel(
    rows, capacity, span, q_ref, key_ref, value_ref, head_gain_ref, routed_ref, weight_ref, residual_ref, gain_ref, out_weight, shared_gate, shared_up, shared_down, expert_gate,
    expert_up, expert_down, out_ref, kv_ref, heads_ref, meta_ref, held, masked, acc, carry, q_up_send, q_up_recv, q_side_send, q_side_recv, head_rows, meta_all, slots, place, mix, gathered, parts, outgoing, arrived, returned, chained, landed,
    base, gate_sum, up_sum, hidden, w_out, w_sgate, w_sup, w_sdown, w_gate, w_up, w_down, w_sem, head_send, head_recv, meta_send,
    meta_recv, up_send, down_send, block_recv, go_send, go_recv, back_send, back_recv, near_send, near_recv, chain_send, chain_recv,
    far_send, far_recv):
    me = lax.axis_index("sp")
    tp = lax.axis_index("tp")
    row, col = me // COLUMNS, me % COLUMNS
    tp_size = head_rows.shape[0]
    group = COLUMNS * tp_size
    mine = col * tp_size + tp
    _, chunks, _, block_rows, width = outgoing.shape
    local = gate_sum.shape[0]
    count = residual_ref.shape[0]
    picks = routed_ref.shape[0]
    total = group * block_rows
    reach = rows // 2
    half = row // reach
    near_first, far_first = half * reach, (1 - half) * reach
    outward = (1 - half) * (reach - 1 - row) + half * (row - reach)
    inner_row = row + 1 - 2 * half
    relays = half * ((2 * reach - 2 - outward) // reach)
    bounds = [(e * span // PACK * PACK, round_up((e + 1) * span, PACK)) for e in range(local)]

    loads = []
    for index, (source, target) in enumerate((
            (out_weight, w_out), (shared_gate, w_sgate), (shared_up, w_sup), (shared_down, w_sdown),
            (expert_gate, w_gate), (expert_up, w_up), (expert_down, w_down))):
        loads.append(pltpu.make_async_copy(source, target, w_sem.at[index]))
        loads[-1].start()

    peers = []
    for across in range(COLUMNS - 1, -1, -1):
        for step in list(range(tp_size // 2, tp_size)) + list(range(tp_size // 2)):
            if across or step:
                peers.append(((col + across) % COLUMNS, (tp + step) % tp_size))

    def device(at_row, at_col, at_tp):
        return {"sp": at_row * COLUMNS + at_col, "tp": at_tp}

    def every(ref, semaphore):
        return pltpu.make_async_remote_copy(
            src_ref=ref, dst_ref=ref, send_sem=semaphore, recv_sem=semaphore, device_id=device(row, COLUMNS - 1 - col, tp),
            device_id_type=MESH)

    barrier = pltpu.get_barrier_semaphore()
    for at_col, at_tp in peers:
        pl.semaphore_signal(barrier, inc=1, device_id=device(row, at_col, at_tp), device_id_type=MESH)
    for step in range(1, rows):
        pl.semaphore_signal(barrier, inc=1, device_id=device((row + step) % rows, col, tp), device_id_type=MESH)
    pl.semaphore_wait(barrier, len(peers) + rows - 1)

    kv_ref[:, : key_ref.shape[1]] = key_ref[...]
    kv_ref[:, key_ref.shape[1] :] = value_ref[...]
    meta_ref[:picks, :] = routed_ref[...].astype(jnp.float32)
    meta_ref[picks:, :] = weight_ref[...]
    meta_all[row] = meta_ref[...]

    def meta_copy(to, source):
        return pltpu.make_async_remote_copy(
            src_ref=meta_ref, dst_ref=meta_all.at[source], send_sem=meta_send, recv_sem=meta_recv,
            device_id=device(to, col, tp), device_id_type=MESH)

    for step in range(1, rows):
        meta_copy((row + step) % rows, row).start()
    attention_step(
        rows, q_ref, kv_ref, head_gain_ref, heads_ref, held, masked, acc, carry, q_up_send, q_up_recv, q_side_send, q_side_recv)

    def head_copy(to, source):
        return pltpu.make_async_remote_copy(
            src_ref=heads_ref.at[pl.ds(pl.multiple_of(to * count, count), count), :],
            dst_ref=head_rows.at[source], send_sem=head_send, recv_sem=head_recv,
            device_id=device(row, col, to), device_id_type=MESH)

    for step in range(1, tp_size):
        head_copy((tp + step) % tp_size, tp).start()
    head_rows[tp] = heads_ref[pl.ds(pl.multiple_of(tp * count, count), count), :]

    def up_copy(chunk, block):
        return pltpu.make_async_remote_copy(
            src_ref=gathered.at[chunk, block], dst_ref=gathered.at[chunk, block], send_sem=up_send.at[block],
            recv_sem=block_recv.at[chunk, block], device_id=device(row + 1, col, tp), device_id_type=MESH)

    def down_copy(chunk, block):
        return pltpu.make_async_remote_copy(
            src_ref=gathered.at[chunk, block], dst_ref=gathered.at[chunk, block], send_sem=down_send.at[block],
            recv_sem=block_recv.at[chunk, block], device_id=device(row - 1, col, tp), device_id_type=MESH)

    def from_below(chunk, block):
        up_copy(chunk, block).wait_recv()

        @pl.when(row < rows - 1)
        def _():
            up_copy(chunk, block).start()

    def from_above(chunk, block):
        down_copy(chunk, block).wait_recv()

        @pl.when(row > 0)
        def _():
            down_copy(chunk, block).start()

    def gather_near(chunk):
        for depth in range(1, reach):
            @pl.when(row - depth >= near_first)
            def _():
                from_below(chunk, row - depth)

            @pl.when(row + depth < near_first + reach)
            def _():
                from_above(chunk, row + depth)

    def gather_far(chunk):
        for depth in range(1, rows):
            @pl.when((row - depth >= 0) & (row - depth < near_first))
            def _():
                from_below(chunk, row - depth)

            @pl.when((row + depth >= near_first + reach) & (row + depth < rows))
            def _():
                from_above(chunk, row + depth)

    def go_copy(part, chunk, peer, source):
        at_col, at_tp = peer
        return pltpu.make_async_remote_copy(
            src_ref=outgoing.at[part, chunk, at_col * tp_size + at_tp], dst_ref=arrived.at[part, chunk, source],
            send_sem=go_send.at[part], recv_sem=go_recv.at[part, chunk],
            device_id=device(row, at_col, at_tp), device_id_type=MESH)

    def back_copy(part, chunk, peer, source):
        at_col, at_tp = peer
        return pltpu.make_async_remote_copy(
            src_ref=outgoing.at[part, chunk, at_col * tp_size + at_tp], dst_ref=returned.at[part, chunk, source],
            send_sem=back_send, recv_sem=back_recv.at[part, chunk],
            device_id=device(row, at_col, at_tp), device_id_type=MESH)

    def near_copy(chunk, block, source):
        return pltpu.make_async_remote_copy(
            src_ref=parts.at[chunk, block], dst_ref=landed.at[chunk, source - near_first],
            send_sem=near_send, recv_sem=near_recv.at[chunk],
            device_id=device(block, col, tp), device_id_type=MESH)

    def chain_copy(chunk, index):
        return pltpu.make_async_remote_copy(
            src_ref=parts.at[chunk, far_first + index], dst_ref=chained.at[chunk, index],
            send_sem=chain_send, recv_sem=chain_recv.at[chunk],
            device_id=device(inner_row, col, tp), device_id_type=MESH)

    def far_copy(chunk, index):
        return pltpu.make_async_remote_copy(
            src_ref=parts.at[chunk, far_first + index], dst_ref=landed.at[chunk, reach],
            send_sem=far_send, recv_sem=far_recv.at[chunk],
            device_id=device(far_first + index, col, tp), device_id_type=MESH)

    def dispatch(part, chunk):
        first_block = near_first if part == 0 else far_first
        tokens = gathered[chunk, pl.ds(first_block, reach)].reshape(reach * count, width)
        rows_out = jnp.dot(place[part], tokens, preferred_element_type=jnp.float32).astype(jnp.bfloat16)
        outgoing[part, chunk] = rows_out.reshape(group, block_rows, width)
        arrived[part, chunk, mine] = outgoing[part, chunk, mine]
        for peer in peers:
            go_copy(part, chunk, peer, mine).start()

    def enter(part, chunk):
        every(arrived.at[part, chunk, pl.ds(0, group - 1)], go_recv.at[part, chunk]).wait_recv()
        deep = pl.ds(pl.multiple_of(chunk * width, width), width)
        for expert, (low, high) in enumerate(bounds):
            block = arrived[part, chunk, :, low:high, :].reshape(group * (high - low), width)
            gate_sum[expert] += jnp.dot(block, w_gate[expert, deep, :], preferred_element_type=jnp.float32)
            up_sum[expert] += jnp.dot(block, w_up[expert, deep, :], preferred_element_type=jnp.float32)

    def activate(part):
        for expert in range(local):
            gate = gate_sum[expert]
            hidden[part, expert] = (gate / (1.0 + jnp.exp(-gate)) * up_sum[expert]).astype(jnp.bfloat16)

    def leave(part, chunk):
        wide = pl.ds(pl.multiple_of(chunk * width, width), width)
        downs = [
            jnp.dot(hidden[part, expert], w_down[expert, :, wide], preferred_element_type=jnp.float32).reshape(group, high - low, width)
            for expert, (low, high) in enumerate(bounds)]
        inside = lax.broadcasted_iota(jnp.int32, (1, PACK, 1), 1)
        for tile in range(0, block_rows, PACK):
            value = None
            for expert, (low, high) in enumerate(bounds):
                if low <= tile < high:
                    piece = downs[expert][:, tile - low : tile - low + PACK, :]
                    value = piece if value is None else jnp.where(inside + tile >= expert * span, piece, value)
            outgoing[part, chunk, :, tile : tile + PACK, :] = value.astype(jnp.bfloat16)
        returned[part, chunk, mine] = outgoing[part, chunk, mine]
        for peer in peers:
            back_copy(part, chunk, peer, mine).start()

    def combine(part, chunk):
        every(returned.at[part, chunk, pl.ds(0, group - 1)], back_recv.at[part, chunk]).wait_recv()
        return returned[part, chunk].reshape(total, width)

    def combine_near(chunk):
        results = combine(0, chunk)
        for step in range(1, reach):
            block = near_first + (row - near_first + step) % reach
            parts[chunk, block] = jnp.dot(mix[block], results, preferred_element_type=jnp.float32).astype(jnp.bfloat16)
        base[chunk] += jnp.dot(mix[row], results, preferred_element_type=jnp.float32)
        for step in range(1, reach):
            near_copy(chunk, near_first + (row - near_first + step) % reach, row).start()

    def combine_far(chunk):
        results = combine(1, chunk)
        for index in range(reach):
            block = far_first + index
            parts[chunk, block] = jnp.dot(mix[block], results, preferred_element_type=jnp.float32).astype(jnp.bfloat16)

        @pl.when(outward == reach - 1)
        def _():
            onward(chunk)

    def onward(chunk):
        for index in range(reach):
            @pl.when(outward > 0)
            def _():
                chain_copy(chunk, index).start()

            @pl.when(outward == 0)
            def _():
                far_copy(chunk, index).start()

    def fold(chunk):
        @pl.when(outward < reach - 1)
        def _():
            every(chained.at[chunk], chain_recv.at[chunk]).wait_recv()
            for index in range(reach):
                block = far_first + index
                parts[chunk, block] = (
                    parts[chunk, block].astype(jnp.float32) + chained[chunk, index].astype(jnp.float32)).astype(jnp.bfloat16)
            onward(chunk)

    def loop(first, last, step):
        def one(index, unused):
            step(index)
            return unused

        lax.fori_loop(first, last, one, 0)

    loads[0].wait()
    every(head_rows.at[pl.ds(0, tp_size - 1)], head_recv).wait_recv()
    token_heads = jnp.concatenate([head_rows[source] for source in range(tp_size)], axis=1)
    branch = jnp.dot(token_heads, w_out[...], preferred_element_type=jnp.float32)
    stream = (residual_ref[...].astype(jnp.float32) + branch).astype(jnp.bfloat16).astype(jnp.float32)
    inverse = lax.rsqrt(jnp.mean(stream * stream, axis=1, keepdims=True) + EPSILON)
    normed = (stream * inverse * gain_ref[...]).astype(jnp.bfloat16)
    for chunk in range(chunks):
        columns = slice(chunk * width, (chunk + 1) * width)
        base[chunk] = stream[:, columns]
        gathered[chunk, row] = normed[:, columns]

    def send_own(chunk):
        @pl.when(row < rows - 1)
        def _():
            up_copy(chunk, row).start()

        @pl.when(row > 0)
        def _():
            down_copy(chunk, row).start()

    loop(0, chunks, send_own)
    every(meta_all.at[pl.ds(0, rows - 1)], meta_recv).wait_recv()
    expert_place = lax.broadcasted_iota(jnp.int32, (group * local, count), 0).astype(jnp.float32)
    slot_place = lax.broadcasted_iota(jnp.int32, (total, count), 0).astype(jnp.float32)
    before = lax.broadcasted_iota(jnp.int32, (count, count), 0)
    after = lax.broadcasted_iota(jnp.int32, (count, count), 1)
    earlier = (before < after).astype(jnp.bfloat16)
    lowest = (row * (group * local)).astype(jnp.float32)
    for part in range(2):
        for index in range(reach):
            block = (near_first if part == 0 else far_first) + index
            meta = meta_all[block]
            chosen = [meta[k : k + 1, :] - lowest for k in range(picks)]
            tables = [jnp.where(expert_place == chosen[k], 1.0, 0.0) for k in range(picks)]
            tally = jnp.dot(sum(tables).astype(jnp.bfloat16), earlier, preferred_element_type=jnp.float32)
            placed = jnp.zeros((total, count), jnp.float32)
            for k in range(picks):
                ranking = jnp.sum(tables[k] * tally, axis=0, keepdims=True)
                inside = (chosen[k] >= 0.0) & (chosen[k] < float(group * local))
                owner = jnp.floor(chosen[k] * (1.0 / local))
                start = owner * float(block_rows) + (chosen[k] - owner * float(local)) * float(span)
                slot = jnp.where(inside, start + (index * capacity + ranking), -1.0)
                slots[block, k : k + 1, :] = slot
                placed = jnp.where(slot_place == slot, 1.0, placed)
            place[part, :, index * count : (index + 1) * count] = placed.astype(jnp.bfloat16)

    for block in range(rows):
        weighed = jnp.zeros((total, count), jnp.float32)
        for k in range(picks):
            slot = slots[block, k : k + 1, :]
            weighed = jnp.where(slot_place == slot, meta_all[block, picks + k : picks + k + 1, :], weighed)
        mix[block] = weighed.T.astype(jnp.bfloat16)

    gate_sum[...] = jnp.zeros_like(gate_sum)
    up_sum[...] = jnp.zeros_like(up_sum)
    for load in loads[1:4]:
        load.wait()
    shared = jnp.dot(normed, w_sgate[...], preferred_element_type=jnp.float32)
    shared = shared / (1.0 + jnp.exp(-shared)) * jnp.dot(normed, w_sup[...], preferred_element_type=jnp.float32)
    shared = shared.astype(jnp.bfloat16)
    for chunk in range(chunks):
        columns = slice(chunk * width, (chunk + 1) * width)
        base[chunk] += jnp.dot(shared, w_sdown[:, columns], preferred_element_type=jnp.float32)

    def near_step(chunk):
        gather_near(chunk)
        dispatch(0, chunk)

        @pl.when(relays == 1)
        def _():
            gather_far(chunk)

    loop(0, chunks, near_step)
    for load in loads[4:]:
        load.wait()

    split = chunks // 2

    def far_step(chunk):
        @pl.when(relays == 0)
        def _():
            gather_far(chunk)

        dispatch(1, chunk)

        @pl.when(chunk < split)
        def _():
            enter(0, 2 * chunk)
            enter(0, 2 * chunk + 1)

        @pl.when(chunk == split)
        def _():
            activate(0)
            gate_sum[...] = jnp.zeros_like(gate_sum)
            up_sum[...] = jnp.zeros_like(up_sum)

        @pl.when(chunk >= split)
        def _():
            enter(1, chunk - split)

    loop(0, chunks, far_step)
    every(outgoing.at[0, :, pl.ds(0, group - 1)], go_send.at[0]).wait_send()
    loop(0, FIRST, lambda chunk: leave(0, chunk))
    loop(chunks - split, chunks, lambda chunk: enter(1, chunk))
    activate(1)
    every(outgoing.at[1, :, pl.ds(0, group - 1)], go_send.at[1]).wait_send()

    loop(0, AHEAD, lambda chunk: leave(1, chunk))

    def far_back(index):
        @pl.when(index + AHEAD < chunks)
        def _():
            leave(1, index + AHEAD)

        @pl.when(index + AHEAD >= chunks)
        def _():
            leave(0, index + AHEAD - chunks + FIRST)

        combine_far(index)

        @pl.when(index >= LAG)
        def _():
            fold(index - LAG)

    loop(0, FIRST, combine_near)
    loop(0, chunks, far_back)

    def close(chunk):
        value = base[chunk]
        far_copy(chunk, 0).wait_recv()
        value += landed[chunk, reach].astype(jnp.float32)
        every(landed.at[chunk, pl.ds(0, reach - 1)], near_recv.at[chunk]).wait_recv()
        for step in range(1, reach):
            source = near_first + (row - near_first + step) % reach
            value += landed[chunk, source - near_first].astype(jnp.float32)
        out_ref[:, pl.ds(pl.multiple_of(chunk * width, width), width)] = value.astype(out_ref.dtype)

    def near_back(index):
        @pl.when(index + AHEAD < chunks)
        def _():
            leave(0, index + AHEAD)

        combine_near(index)
        turn = index - FIRST

        @pl.when((turn >= 1) & (turn <= LAG))
        def _():
            fold(chunks - LAG + turn - 1)

        @pl.when(turn >= LAG)
        def _():
            close(turn - LAG)

    loop(FIRST, chunks, near_back)
    loop(chunks - FIRST - LAG, chunks, close)
    every(outgoing.at[:, :, pl.ds(0, group - 1)], back_send).wait_send()
    every(parts.at[:, pl.ds(0, reach - 1)], near_send).wait_send()

    @pl.when(outward > 0)
    def _():
        every(parts.at[:, pl.ds(0, reach)], chain_send).wait_send()

    @pl.when(outward == 0)
    def _():
        every(parts.at[:, pl.ds(0, reach)], far_send).wait_send()

    @pl.when(row < rows - 1)
    def _():
        loop(0, row + 1, lambda block: every(gathered.at[:, block], up_send.at[block]).wait_send())

    @pl.when(row > 0)
    def _():
        loop(row, rows, lambda block: every(gathered.at[:, block], down_send.at[block]).wait_send())

    every(head_rows.at[pl.ds(0, tp_size - 1)], head_send).wait_send()
    every(meta_all.at[pl.ds(0, rows - 1)], meta_send).wait_send()


def layer(
    queries, key_heads, value_heads, head_gain, residual, out_weight, norm_gain, shared_gate, shared_up, shared_down, expert_gate, expert_up, expert_down,
    routed_experts, route_weights):
    count, picks = routed_experts.shape
    model = residual.shape[1]
    sp_size, tp_size = lax.axis_size("sp"), lax.axis_size("tp")
    rows, group = sp_size // COLUMNS, COLUMNS * tp_size
    reach = rows // 2
    local, _, inner = expert_gate.shape
    expert_count = local * sp_size * tp_size
    capacity = max(2, 3 * count * picks // (2 * expert_count))
    span = round_up(reach * capacity, 8)
    block_rows = round_up(local * span, PACK)
    total = group * block_rows
    wide = max(round_up((e + 1) * span, PACK) - e * span // PACK * PACK for e in range(local))
    width = model // CHUNKS
    seq, head_width = queries.shape
    heads = head_width // HEAD_DIM
    pieces = max(seq // TILE, 1) * SPLIT
    vmem = pl.BlockSpec(memory_space=pltpu.VMEM)
    hbm = pl.BlockSpec(memory_space=pl.ANY)
    half = jnp.bfloat16

    return pl.pallas_call(
        functools.partial(layer_kernel, rows, capacity, span),
        out_shape=jax.ShapeDtypeStruct((count, model), half),
        in_specs=[vmem] * 8 + [hbm] * 7,
        out_specs=vmem,
        scratch_shapes=[
            pltpu.VMEM((seq, 2 * head_width), half),
            pltpu.VMEM((seq, head_width), half),
            pltpu.VMEM((2 * picks, count), jnp.float32),
            pltpu.VMEM((sp_size, seq, 2 * head_width), half),
            pltpu.VMEM((heads * seq, head_width), half),
            pltpu.VMEM((heads * seq, head_width), jnp.float32),
            pltpu.VMEM((heads * seq, 1), jnp.float32),
            *[pltpu.SemaphoreType.DMA((rows,)), pltpu.SemaphoreType.DMA((rows, pieces))] * 2,
            pltpu.VMEM((tp_size, count, head_width), half),
            pltpu.VMEM((rows, 2 * picks, count), jnp.float32),
            pltpu.VMEM((rows, 2 * picks, count), jnp.float32),
            pltpu.VMEM((2, total, reach * count), half),
            pltpu.VMEM((rows, count, total), half),
            pltpu.VMEM((CHUNKS, rows, count, width), half),
            pltpu.VMEM((CHUNKS, rows, count, width), half),
            pltpu.VMEM((2, CHUNKS, group, block_rows, width), half),
            pltpu.VMEM((2, CHUNKS, group, block_rows, width), half),
            pltpu.VMEM((2, CHUNKS, group, block_rows, width), half),
            pltpu.VMEM((CHUNKS, reach, count, width), half),
            pltpu.VMEM((CHUNKS, reach + 1, count, width), half),
            pltpu.VMEM((CHUNKS, count, width), jnp.float32),
            pltpu.VMEM((local, group * wide, inner), jnp.float32),
            pltpu.VMEM((local, group * wide, inner), jnp.float32),
            pltpu.VMEM((2, local, group * wide, inner), half),
            pltpu.VMEM(out_weight.shape, half),
            pltpu.VMEM(shared_gate.shape, half),
            pltpu.VMEM(shared_up.shape, half),
            pltpu.VMEM(shared_down.shape, half),
            pltpu.VMEM(expert_gate.shape, half),
            pltpu.VMEM(expert_up.shape, half),
            pltpu.VMEM(expert_down.shape, half),
            pltpu.SemaphoreType.DMA((7,)),
            *[pltpu.SemaphoreType.DMA] * 4,
            *[pltpu.SemaphoreType.DMA((rows,))] * 2,
            pltpu.SemaphoreType.DMA((CHUNKS, rows)),
            pltpu.SemaphoreType.DMA((2,)),
            pltpu.SemaphoreType.DMA((2, CHUNKS)),
            pltpu.SemaphoreType.DMA,
            pltpu.SemaphoreType.DMA((2, CHUNKS)),
            *[pltpu.SemaphoreType.DMA, pltpu.SemaphoreType.DMA((CHUNKS,))] * 3,
        ],
        compiler_params=pltpu.CompilerParams(collective_id=0, has_side_effects=True, vmem_limit_bytes=VMEM_LIMIT),
        name="layer",
    )(queries, key_heads, value_heads, head_gain.reshape(1, head_width), routed_experts.T, route_weights.T, residual, norm_gain.reshape(1, model), out_weight, shared_gate, shared_up, shared_down,
      expert_gate, expert_up, expert_down)


def body(
    queries,
    key_heads,
    value_heads,
    head_gain,
    residual,
    out_weight,
    norm_gain,
    shared_gate,
    shared_up,
    shared_down,
    expert_gate,
    expert_up,
    expert_down,
    routed_experts,
    route_weights,
):
    return layer(
        queries, key_heads, value_heads, head_gain, residual, out_weight, norm_gain, shared_gate, shared_up, shared_down,
        expert_gate, expert_up, expert_down, routed_experts, route_weights)


def solution(mesh):
    return jax.shard_map(
        body,
        mesh=mesh,
        in_specs=(
            P("sp", "tp"),
            P("sp", "tp"),
            P("sp", "tp"),
            P("tp"),
            P(("sp", "tp"), None),
            P(),
            P(),
            P(),
            P(),
            P(),
            P(("sp", "tp"), None, None),
            P(("sp", "tp"), None, None),
            P(("sp", "tp"), None, None),
            P(("sp", "tp"), None),
            P(("sp", "tp"), None),
        ),
        out_specs=P(("sp", "tp"), None),
        check_vma=False,
    )
```
